128 devices in a mesh: ep: 64 (over z, y, x), tp: 2 (over core).
Axes of the slice: x: 4, y: 4, z: 4, core: 2. Of those that a mesh axis runs over, the one named last changes fastest.
Arguments:
- tokens: bfloat16 [1024, 2048], P('ep'), may hold values from -6 to 6
- state: float32 [1024, 8, 128, 128], P('ep', 'tp'), may hold values from -6 to 6
- mix_gain: float32 [2048], replicated, may hold values from 0.1 to 1.9
- moe_gain: float32 [2048], replicated, may hold values from 0.1 to 1.9
- head_gain: float32 [128], replicated, may hold values from 0.1 to 1.9
- w_forget: bfloat16 [2048, 1024], P(None, 'tp'), may hold values from -0.125 to 0.125
- w_query: bfloat16 [2048, 1024], P(None, 'tp'), may hold values from -0.125 to 0.125
- w_input: bfloat16 [2048, 1024], P(None, 'tp'), may hold values from -0.125 to 0.125
- w_outgate: bfloat16 [2048, 1024], P(None, 'tp'), may hold values from -0.125 to 0.125
- lower_bound: float32 [1024], P('tp'), may hold values from 0 to 0.9
- w_mix_out: bfloat16 [1024, 2048], P('tp'), may hold values from -0.1875 to 0.1875
- routes: int32 [1024, 6], P('ep'), may hold values from 0 to 63, all different within a row; in each aligned block of 16 rows (0 to 15, 16 to 31, ...) at most 4 rows name the same one
- route_scores: float32 [1024, 6], P('ep'), may hold values from 0.05 to 1
- expert_gate: bfloat16 [64, 2048, 512], P('ep', None, 'tp'), may hold values from -0.125 to 0.125
- expert_up: bfloat16 [64, 2048, 512], P('ep', None, 'tp'), may hold values from -0.125 to 0.125
- expert_down: bfloat16 [64, 512, 2048], P('ep', 'tp'), may hold values from -0.25 to 0.25
- shared_gate: bfloat16 [2048, 512], P(None, 'tp'), may hold values from -0.125 to 0.125
- shared_up: bfloat16 [2048, 512], P(None, 'tp'), may hold values from -0.125 to 0.125
- shared_down: bfloat16 [512, 2048], P('tp'), may hold values from -0.25 to 0.25
Outputs:
- layer_out: bfloat16 [1024, 2048], P('ep', 'tp')
- new_state: float32 [1024, 8, 128, 128], P('ep', 'tp')
The draws below stay inside these ranges and needn't reach their ends.
Inputs may be any that keep to these rules, and one draw needn't show every extreme that they name: `routes`: each token names 6 different experts. Among the tokens of one index of ep no expert is named by more than 4 tokens, and in every draw some expert is named by exactly 4 tokens of some index of ep.
All inputs are finite; a program needn't handle non-finite values.
Results may differ from the reference program's by a relative error of at most 0.017.
Values may be sent and summed in bfloat16 or wider, within the bound.
A program may use at most 128 MiB of HBM per device.

```python
import math
import jax
import jax.numpy as jnp
import numpy as np
from jax import lax

D = 2048
HEADS = 8
HEAD_KEY = 128
HEAD_VALUE = 128
FE = 512
TOP_K = 6
S_DEV = 16
EXPERTS = 64
SEQS = 1024
CAP = 4
N_EP = 64


def steps_of(own_key, shape, pieces, smallest, largest):
    level = 1.0
    for position, parts in pieces:
        draws = jax.random.uniform(jax.random.fold_in(jax.random.fold_in(own_key, 6), position), (parts,), jnp.float32, smallest / len(pieces), largest / len(pieces))
        level = level * jnp.repeat(jnp.exp(draws), shape[position] // parts).reshape((-1,) + (1,) * (len(shape) - 1 - position))
    return level


def deal_out(own_key, own, number, rows, number_of, top, bound, slope):
    order = jax.random.permutation(own_key, number_of)
    heavy_load, usual = shares(number_of, rows * top, bound, slope, True), shares(number_of, rows * top, bound, slope, False)
    places = jnp.arange(number_of)

    def named(sizes, offset_by):
        used = int((sizes > 0).sum())
        fixed = max(1, used // 4)
        moved = fixed + (places - fixed + offset_by * (used - fixed)) % max(1, number_of - fixed)
        return jnp.zeros((number_of,), jnp.int32).at[order[jnp.where(places < fixed, places, moved)]].set(jnp.asarray(sizes, jnp.int32))

    sizes = jnp.where(number % 4 == 0, named(heavy_load, number // 4), named(usual, number - number // 4 - 1))
    mixed = jax.random.permutation(jax.random.fold_in(own, 3), number_of)
    giver, taker = mixed[0:number_of // 2 * 2:2], mixed[1:number_of // 2 * 2:2]
    margin = jnp.minimum(sizes[giver] - 1, bound - sizes[taker]) // 2
    margin = jnp.where((giver == order[0]) | (taker == order[0]) | (sizes[taker] == 0), 0, jnp.maximum(margin, 0))
    moved = jax.random.randint(jax.random.fold_in(own, 4), (number_of // 2,), 0, 1 << 20) % (margin + 1)
    sizes = sizes.at[giver].add(-moved).at[taker].add(moved)
    items = jnp.searchsorted(jnp.cumsum(sizes), jnp.arange(rows * top), side="right").astype(jnp.int32)
    grid = items.reshape(top, rows).T
    grid = grid[jax.random.permutation(jax.random.fold_in(own, 1), rows)]
    offset_by = jax.random.randint(jax.random.fold_in(own, 2), (rows, 1), 0, top)
    return jnp.take_along_axis(grid, (jnp.arange(top)[None, :] + offset_by) % top, axis=1)


def shares(number_of, total, most, slope, full):
    loads = [(1 << 20) // math.isqrt(standing ** slope) + 1 for standing in range(1, number_of + 1)]
    largest = most if full else min(most, max(-(-total // number_of), total * loads[0] // sum(loads)))
    least = 1 if total - largest >= number_of - 1 else 0
    counts, spare = [largest] + [least] * (number_of - 1), total - largest - least * (number_of - 1)
    while spare > 0:
        movable = [i for i in range(1, number_of) if counts[i] < largest] or [i for i in range(1, number_of) if counts[i] < most]
        mass, remaining = sum([loads[i] for i in movable]), spare
        for i in movable:
            extra = min(most - counts[i], max(1, remaining * loads[i] // mass), spare)
            counts[i] = counts[i] + extra
            spare = spare - extra
    return np.array(counts)


def centred(stream_key, shape, deviation, bound, shards=(), kind=jnp.bfloat16):
    array = jax.random.normal(stream_key, shape, jnp.float32) * deviation
    if len(shards) > 0:
        array = steps_of(stream_key, shape, shards, -0.22, 0.18) * array
    return jnp.clip(array, min=-bound, max=bound).astype(kind)


def setup_inputs(seed: int = 0) -> dict:
    keys = jax.random.split(jax.random.key(seed), 20)
    tokens = centred(keys[0], (SEQS, D), 1.0, 6.0, ((0, 64),))
    state = centred(keys[1], (SEQS, HEADS, HEAD_KEY, HEAD_VALUE), 1.0, 6.0, ((0, 64), (1, 2)), jnp.float32)
    mix_gain = jnp.clip(1.0 + 0.18 * jax.random.normal(keys[2], (D,), jnp.float32), 0.1, 1.9)
    moe_gain = jnp.clip(1.0 + 0.18 * jax.random.normal(keys[3], (D,), jnp.float32), 0.1, 1.9)
    head_gain = jnp.clip(1.0 + 0.18 * jax.random.normal(keys[4], (HEAD_VALUE,), jnp.float32), 0.1, 1.9)
    w_forget = centred(keys[5], (D, HEADS * HEAD_KEY), D ** -0.5, 0.125, ((1, 2),))
    w_query = centred(keys[6], (D, HEADS * HEAD_KEY), D ** -0.5, 0.125, ((1, 2),))
    w_input = centred(keys[7], (D, HEADS * HEAD_VALUE), D ** -0.5, 0.125, ((1, 2),))
    w_outgate = centred(keys[8], (D, HEADS * HEAD_VALUE), D ** -0.5, 0.125, ((1, 2),))
    lower_bound = jnp.clip(0.9 * jax.random.uniform(keys[9], (HEADS * HEAD_KEY,), jnp.float32) ** steps_of(keys[9], (HEADS * HEAD_KEY,), ((0, 2),), -0.2, 0.2), 0.0, 0.9)
    w_mix_out = centred(keys[10], (HEADS * HEAD_VALUE, D), (HEADS * HEAD_VALUE) ** -0.5, 0.1875, ((0, 2),))
    routes_keys = jax.random.split(jax.random.fold_in(keys[11], 1), SEQS // S_DEV)
    routes_turns = jax.random.permutation(jax.random.fold_in(keys[11], 3), SEQS // S_DEV)
    routes = jax.vmap(lambda own, number: deal_out(jax.random.fold_in(keys[11], 2), own, number, S_DEV, EXPERTS, TOP_K, CAP, 2))(routes_keys, routes_turns).reshape((SEQS, TOP_K))
    route_scores = jnp.clip(0.05 + 0.95 * jax.random.uniform(keys[12], (SEQS, TOP_K), jnp.float32) ** steps_of(keys[12], (SEQS, TOP_K), ((0, 64),), -0.2, 0.2), 0.05, 1.0)
    expert_gate = centred(keys[13], (EXPERTS, D, FE), D ** -0.5, 0.125, ((0, 64), (2, 2)))
    expert_up = centred(keys[14], (EXPERTS, D, FE), D ** -0.5, 0.125, ((0, 64), (2, 2)))
    expert_down = centred(keys[15], (EXPERTS, FE, D), FE ** -0.5, 0.25, ((0, 64), (1, 2)))
    shared_gate = centred(keys[16], (D, FE), D ** -0.5, 0.125, ((1, 2),))
    shared_up = centred(keys[17], (D, FE), D ** -0.5, 0.125, ((1, 2),))
    shared_down = centred(keys[18], (FE, D), FE ** -0.5, 0.25, ((0, 2),))
    return dict(tokens=tokens, state=state, mix_gain=mix_gain, moe_gain=moe_gain, head_gain=head_gain, w_forget=w_forget, w_query=w_query, w_input=w_input, w_outgate=w_outgate, lower_bound=lower_bound, w_mix_out=w_mix_out, routes=routes, route_scores=route_scores, expert_gate=expert_gate, expert_up=expert_up, expert_down=expert_down, shared_gate=shared_gate, shared_up=shared_up, shared_down=shared_down)


epsilon = 1e-06
routed_scale = 2.5

def rms_scale(values, gain):
    return values * lax.rsqrt(lax.optimization_barrier(jnp.mean(values * values, axis=-1, keepdims=True)) + epsilon) * gain

def rounded(values):
    return lax.optimization_barrier(values.astype(jnp.bfloat16)).astype(jnp.float32)

def halves_sum(operand, weight, split_at):
    first = jnp.dot(operand[:, :split_at], weight[:split_at], preferred_element_type=jnp.float32)
    second = jnp.dot(operand[:, split_at:], weight[split_at:], preferred_element_type=jnp.float32)
    return (rounded(first) + rounded(second)).astype(jnp.bfloat16)

def reference(tokens, state, mix_gain, moe_gain, head_gain, w_forget, w_query, w_input, w_outgate, lower_bound, w_mix_out, routes, route_scores, expert_gate, expert_up, expert_down, shared_gate, shared_up, shared_down):
    seq_count = tokens.shape[0]
    tokens_wide = tokens.astype(jnp.float32)
    normed = rms_scale(tokens_wide, mix_gain).astype(jnp.bfloat16)
    forget_pre = jnp.dot(normed, w_forget, preferred_element_type=jnp.float32).reshape(seq_count, HEADS, HEAD_KEY)
    query = jax.nn.silu(jnp.dot(normed, w_query, preferred_element_type=jnp.float32)).reshape(seq_count, HEADS, HEAD_KEY)
    input_val = jnp.dot(normed, w_input, preferred_element_type=jnp.float32).reshape(seq_count, HEADS, HEAD_VALUE)
    gate_pre = jnp.dot(normed, w_outgate, preferred_element_type=jnp.float32).reshape(seq_count, HEADS, HEAD_VALUE)
    bound_rows = lower_bound.reshape(HEADS, HEAD_KEY)
    forget = bound_rows + (1.0 - bound_rows) * jax.nn.sigmoid(forget_pre)
    key_gate = (1.0 - bound_rows) * jax.nn.sigmoid(-forget_pre)
    new_state = forget[..., None] * state + key_gate[..., None] * input_val[:, :, None, :]
    readout = jnp.einsum('shkv,shk->shv', new_state, query, precision=lax.Precision.HIGHEST)
    gated_out = (rms_scale(readout, head_gain) * jax.nn.silu(gate_pre)).astype(jnp.bfloat16)
    gated_out = gated_out.reshape(seq_count, HEADS * HEAD_VALUE)
    mixer_out = halves_sum(gated_out, w_mix_out, HEADS * HEAD_VALUE // 2)
    residual = tokens_wide + mixer_out.astype(jnp.float32)
    moe_rows = rms_scale(residual, moe_gain).astype(jnp.bfloat16)
    weights = route_scores / lax.optimization_barrier(jnp.sum(route_scores, axis=-1, keepdims=True)) * routed_scale
    shared_hidden = (jax.nn.silu(jnp.dot(moe_rows, shared_gate, preferred_element_type=jnp.float32)) * jnp.dot(moe_rows, shared_up, preferred_element_type=jnp.float32)).astype(jnp.bfloat16)
    shared_out = halves_sum(shared_hidden, shared_down, FE // 2)
    flat_routes = routes.reshape(-1)
    slot_count = N_EP * CAP
    rows_repeated = jnp.repeat(moe_rows, TOP_K, axis=0)

    def one_expert(totals, inputs):
        gate_w, up_w, down_w, expert_id = inputs
        chosen = flat_routes == expert_id
        slot_rank = (jnp.cumsum(chosen.astype(jnp.int32)) - 1).astype(jnp.int32)
        target = jnp.where(chosen, slot_rank, slot_count).astype(jnp.int32)
        buffer = jnp.zeros((slot_count, D), jnp.bfloat16).at[target].set(rows_repeated, mode='drop')
        hidden = (jax.nn.silu(jnp.dot(buffer, gate_w, preferred_element_type=jnp.float32)) * jnp.dot(buffer, up_w, preferred_element_type=jnp.float32)).astype(jnp.bfloat16)
        result = halves_sum(hidden, down_w, FE // 2)
        picked = result[jnp.clip(slot_rank, 0, slot_count - 1)].astype(jnp.float32)
        return (totals + jnp.where(chosen[:, None], picked, jnp.float32(0.0)), None)
    totals, _ = lax.scan(one_expert, jnp.zeros((seq_count * TOP_K, D), jnp.float32), (expert_gate, expert_up, expert_down, jnp.arange(EXPERTS, dtype=jnp.int32)))
    routed = lax.optimization_barrier(jnp.sum(totals.reshape(seq_count, TOP_K, D) * weights[:, :, None], axis=1))
    layer_out = (residual + routed + shared_out.astype(jnp.float32)).astype(jnp.bfloat16)
    return (layer_out, new_state)
```

```python
import functools

import jax
import jax.numpy as jnp
from jax import lax
from jax.experimental import pallas as pl
from jax.experimental.pallas import tpu as pltpu
from jax.sharding import PartitionSpec as P

epsilon = 1e-06
routed_scale = 2.5
MESH = pl.DeviceIdType.MESH
bf16, f32, i32 = jnp.bfloat16, jnp.float32, jnp.int32


def rms_scale(values, gain):
    return values * lax.rsqrt(jnp.mean(values * values, axis=-1, keepdims=True) + epsilon) * gain


def silu(v):
    return v / (1.0 + jnp.exp(-v))


def dot(a, b):
    return jnp.dot(a, b, preferred_element_type=f32)


def iota(shape, dim):
    return lax.broadcasted_iota(i32, shape, dim)


def toward(ep, off, sign):
    z, y, x = ep // 16, (ep // 4) % 4, ep % 4
    dz, dy, dx = off // 16, (off // 4) % 4, off % 4
    if sign < 0:
        dz, dy, dx = 4 - dz, 4 - dy, 4 - dx
    return ((z + dz) % 4) * 16 + ((y + dy) % 4) * 4 + (x + dx) % 4


def greet_all(ep, tp):
    barrier = pltpu.get_barrier_semaphore()

    def greet(i, c):
        peer = toward(ep, i, 1)
        for t in range(2):
            pl.semaphore_signal(barrier, inc=1, device_id=(peer, t), device_id_type=MESH)
        return c

    lax.fori_loop(1, 64, greet, 0)
    pl.semaphore_signal(barrier, inc=1, device_id=(ep, 1 - tp), device_id_type=MESH)


def await_all():
    pl.semaphore_wait(pltpu.get_barrier_semaphore(), 127)


def route_tables(routes, scores, ep):
    z, y, x = ep // 16, (ep // 4) % 4, ep % 4
    weights = scores / jnp.sum(scores, axis=-1, keepdims=True) * routed_scale
    rz = ((routes >> 4) - z) & 3
    ry = (((routes >> 2) & 3) - y) & 3
    rx = ((routes & 3) - x) & 3
    rel = rz * 16 + ry * 4 + rx
    lanes = iota((16, 64), 1)
    named = jnp.zeros((16, 64), f32)
    weight = jnp.zeros((16, 64), f32)
    for k in range(6):
        hit = rel[:, k : k + 1] == lanes
        named = jnp.where(hit, 1.0, named)
        weight = jnp.where(hit, weights[:, k : k + 1], weight)
    earlier = (iota((16, 16), 1) < iota((16, 16), 0)).astype(bf16)
    rank = dot(earlier, named.astype(bf16))
    code = jnp.where(named > 0.5, rank + 1.0, 0.0)
    return code, weight


def place_rows(code, tp, place_ref):
    spread = (iota((16, 128), 1) % 16 == iota((16, 128), 0)).astype(bf16)
    codes = lax.dot_general(
        code.astype(bf16), spread, (((0,), (0,)), ((), ())), preferred_element_type=f32
    ).astype(bf16)
    for b in range(4):
        grow = (iota((256, 64), 0) // 16 + 16 * b == iota((256, 64), 1)).astype(bf16)
        grown = dot(grow, codes)
        row = iota((256, 128), 0) % 16
        target = (2 * tp + row // 8 + 1).astype(f32)
        fits = (grown == target) & (iota((256, 128), 1) // 16 == row % 8)
        place_ref[pl.ds(256 * b, 256), :] = jnp.where(fits, 1.0, 0.0).astype(bf16)


def combine_rows(code, weight, comb_ref):
    both = jnp.concatenate([code, weight], axis=0).astype(bf16)
    for n in range(8):
        col = iota((64, 256), 1) + 256 * n
        grow = (col // 32 == iota((64, 256), 0)).astype(bf16)
        grown = dot(both, grow)
        col = iota((16, 256), 1)
        slot = ((col // 8) % 4 + 1).astype(f32)
        value = jnp.where(grown[:16] == slot, grown[16:], 0.0)
        for j in range(8):
            comb_ref[pl.ds(16 * j, 16), pl.ds(256 * n, 256)] = jnp.where(
                col % 8 == j, value, 0.0
            ).astype(bf16)


def moe_kernel(
    rows_ref, routes_ref, scores_ref, gate_ref, up_ref, down_ref, out_ref,
    gate_own, up_own, down_own, gate_par, up_par, down_par,
    place, comb, send, recv, xs, ret, back,
    load_sem, push_sem, pull_sem, go_send, go_recv, ret_send, ret_recv,
):
    ep, tp = lax.axis_index("ep"), lax.axis_index("tp")
    partner = (ep, 1 - tp)
    greet_all(ep, tp)
    loads = [
        pltpu.make_async_copy(src.at[0], dst, load_sem.at[i])
        for i, (src, dst) in enumerate(((gate_ref, gate_own), (up_ref, up_own), (down_ref, down_own)))
    ]
    for copy in loads:
        copy.start()
    code, weight = route_tables(routes_ref[...], scores_ref[...], ep)
    place_rows(code, tp, place)
    combine_rows(code, weight, comb)
    await_all()
    pushes = [
        pltpu.make_async_remote_copy(
            src_ref=src.at[0], dst_ref=dst, send_sem=push_sem.at[i], recv_sem=pull_sem.at[i],
            device_id=partner, device_id_type=MESH,
        )
        for i, (src, dst) in enumerate(((gate_ref, gate_par), (up_ref, up_par), (down_ref, down_par)))
    ]
    for copy in pushes:
        copy.start()

    rows = rows_ref[...]
    stacked = jnp.concatenate([rows[:, 256 * j : 256 * (j + 1)] for j in range(8)], axis=0)

    def go(i):
        return pltpu.make_async_remote_copy(
            src_ref=send.at[i], dst_ref=recv.at[i], send_sem=go_send, recv_sem=go_recv,
            device_id=(toward(ep, i, 1), tp), device_id_type=MESH,
        )

    for b in range(4):
        placed = dot(place[pl.ds(256 * b, 256), :], stacked).astype(bf16)
        send[pl.ds(16 * b, 16)] = placed.reshape(16, 16, 256)

        def start(i, c):
            go(i).start()
            return c

        lax.fori_loop(max(1, 16 * b), 16 * b + 16, start, 0)
    recv[0] = send[0]

    def all_of(buf, n):
        return buf.at[pl.ds(0, n)]

    pltpu.make_async_remote_copy(
        src_ref=all_of(send, 63), dst_ref=all_of(recv, 63), send_sem=go_send, recv_sem=go_recv,
        device_id=partner, device_id_type=MESH,
    ).wait()
    for copy in loads:
        copy.wait()
    for copy in pushes:
        copy.wait()

    out_row, in_row = iota((256, 256), 0), iota((256, 256), 1)
    sort = ((out_row // 32 == in_row % 8) & ((out_row // 2) % 16 == in_row // 16)
            & (out_row % 2 == (in_row // 8) % 2)).astype(bf16)
    unsort = ((in_row // 32 == out_row % 8) & ((in_row // 2) % 16 == out_row // 16)
              & (in_row % 2 == (out_row // 8) % 2)).astype(bf16)
    for b in range(4):
        sorted_rows = dot(sort, recv[pl.ds(16 * b, 16)].reshape(256, 256)).astype(bf16)
        for j in range(8):
            xs[pl.ds(32 * b, 32), pl.ds(256 * j, 256)] = sorted_rows[32 * j : 32 * j + 32]
    x = xs[...]
    hidden_own = (silu(dot(x, gate_own[...])) * dot(x, up_own[...])).astype(bf16)
    hidden_par = (silu(dot(x, gate_par[...])) * dot(x, up_par[...])).astype(bf16)
    for n in range(8):
        cols = pl.ds(256 * n, 256)
        xs[:, cols] = (dot(hidden_own, down_own[:, cols]) + dot(hidden_par, down_par[:, cols])).astype(bf16)

    def come(i, h):
        return pltpu.make_async_remote_copy(
            src_ref=ret.at[2 * i + h], dst_ref=back.at[2 * i + tp], send_sem=ret_send, recv_sem=ret_recv,
            device_id=(toward(ep, i, -1), h), device_id_type=MESH,
        )

    for b in range(4):
        tall = jnp.concatenate(
            [
                jnp.concatenate(
                    [xs[pl.ds(32 * b, 32), pl.ds(128 * j + 1024 * h, 128)] for h in range(2)], axis=1
                )
                for j in range(8)
            ],
            axis=0,
        )
        turned = dot(unsort, tall).astype(bf16)
        for i in range(16):
            for h in range(2):
                ret[2 * (16 * b + i) + h] = turned[16 * i : 16 * i + 16, 128 * h : 128 * h + 128]

        def start_back(i, c):
            for h in range(2):
                come(i, h).start()
            return c

        lax.fori_loop(max(1, 16 * b), 16 * b + 16, start_back, 0)
    pltpu.make_async_remote_copy(
        src_ref=ret.at[1 - tp], dst_ref=back.at[tp], send_sem=ret_send, recv_sem=ret_recv,
        device_id=partner, device_id_type=MESH,
    ).start()
    back[tp] = ret[tp]
    pltpu.make_async_remote_copy(
        src_ref=all_of(ret, 127), dst_ref=all_of(back, 127), send_sem=ret_send, recv_sem=ret_recv,
        device_id=partner, device_id_type=MESH,
    ).wait()
    total = dot(comb[...], back[...].reshape(2048, 128))
    for j in range(8):
        out_ref[:, pl.ds(128 * j, 128)] = total[16 * j : 16 * j + 16]


def moe(rows, routes, scores, gate, up, down):
    vm = pl.BlockSpec(memory_space=pltpu.VMEM)
    hbm = pl.BlockSpec(memory_space=pl.ANY)
    dma = pltpu.SemaphoreType.DMA
    return pl.pallas_call(
        moe_kernel,
        name="moe",
        out_shape=jax.ShapeDtypeStruct((16, 1024), f32),
        in_specs=[vm, vm, vm, hbm, hbm, hbm],
        out_specs=vm,
        scratch_shapes=[
            pltpu.VMEM((2048, 256), bf16), pltpu.VMEM((2048, 256), bf16), pltpu.VMEM((256, 2048), bf16),
            pltpu.VMEM((2048, 256), bf16), pltpu.VMEM((2048, 256), bf16), pltpu.VMEM((256, 2048), bf16),
            pltpu.VMEM((1024, 128), bf16), pltpu.VMEM((128, 2048), bf16),
            pltpu.VMEM((64, 16, 256), bf16), pltpu.VMEM((64, 16, 256), bf16), pltpu.VMEM((128, 2048), bf16),
            pltpu.VMEM((128, 16, 128), bf16), pltpu.VMEM((128, 16, 128), bf16),
            dma((3,)), dma((3,)), dma((3,)), dma, dma, dma, dma,
        ],
        compiler_params=pltpu.CompilerParams(
            collective_id=0, has_side_effects=True, vmem_limit_bytes=48 << 20
        ),
    )(rows, routes, scores, gate, up, down)


def total_of_pieces(array, axis):
    tiles = lax.all_gather(array, axis).astype(jnp.float32)
    return tiles.sum(axis=0)


def cut_along(array, dim, devices):
    before, after = (array.shape[:dim], array.shape[dim + 1 :])
    return jnp.moveaxis(array.reshape(*before, devices, -1, *after), dim, 0)


def sent_and_summed(array, axis, dim):
    devices = lax.axis_size(axis)
    tiles = lax.all_to_all(cut_along(array, dim, devices), axis, 0, 0, tiled=True)
    return jnp.sum(tiles.astype(jnp.float32), axis=0)


def laid_out(tiles, dim):
    tiles = jnp.moveaxis(tiles, 0, dim)
    shape = tiles.shape
    return tiles.reshape(*shape[:dim], shape[dim] * shape[dim + 1], *shape[dim + 2 :])


def sent_to_all(array, axis):
    copies = jnp.broadcast_to(array, (lax.axis_size(axis), *array.shape))
    return lax.all_to_all(copies, axis, split_axis=0, concat_axis=0, tiled=True)


def gather_directly(array, axis, dim):
    return laid_out(sent_to_all(array, axis), dim)


def local(
    tokens,
    state,
    mix_gain,
    moe_gain,
    head_gain,
    w_forget,
    w_query,
    w_input,
    w_outgate,
    lower_bound,
    w_mix_out,
    routes,
    route_scores,
    expert_gate,
    expert_up,
    expert_down,
    shared_gate,
    shared_up,
    shared_down,
):
    seqs_here = tokens.shape[0]
    heads_here = state.shape[1]
    key_width = state.shape[2]
    value_width = state.shape[3]
    tokens_wide = tokens.astype(jnp.float32)
    normed = rms_scale(tokens_wide, mix_gain).astype(jnp.bfloat16)
    forget_pre = jnp.dot(normed, w_forget, preferred_element_type=jnp.float32).reshape(
        seqs_here, heads_here, key_width
    )
    query = jax.nn.silu(jnp.dot(normed, w_query, preferred_element_type=jnp.float32)).reshape(
        seqs_here, heads_here, key_width
    )
    input_val = jnp.dot(normed, w_input, preferred_element_type=jnp.float32).reshape(
        seqs_here, heads_here, value_width
    )
    gate_pre = jnp.dot(normed, w_outgate, preferred_element_type=jnp.float32).reshape(
        seqs_here, heads_here, value_width
    )
    bound_rows = lower_bound.reshape(heads_here, key_width)
    forget = bound_rows + (1.0 - bound_rows) * jax.nn.sigmoid(forget_pre)
    key_gate = (1.0 - bound_rows) * jax.nn.sigmoid(-forget_pre)
    new_state = forget[..., None] * state + key_gate[..., None] * input_val[:, :, None, :]
    readout = jnp.einsum("shkv,shk->shv", new_state, query)
    gated_out = (rms_scale(readout, head_gain) * jax.nn.silu(gate_pre)).astype(jnp.bfloat16)
    gated_out = gated_out.reshape(seqs_here, heads_here * value_width)
    partial_value = jnp.dot(gated_out, w_mix_out, preferred_element_type=jnp.float32)
    mixer_out = (
        total_of_pieces(partial_value.astype(jnp.bfloat16), "tp")
        .astype(jnp.float32)
        .astype(jnp.bfloat16)
    )
    residual = tokens_wide + mixer_out.astype(jnp.float32)
    moe_rows = rms_scale(residual, moe_gain).astype(jnp.bfloat16)
    full_width = moe_rows.shape[1]
    half_width = full_width // 2
    tp_index = lax.axis_index("tp")
    shared_hidden = (
        jax.nn.silu(jnp.dot(moe_rows, shared_gate, preferred_element_type=jnp.float32))
        * jnp.dot(moe_rows, shared_up, preferred_element_type=jnp.float32)
    ).astype(jnp.bfloat16)
    shared_part = jnp.dot(shared_hidden, shared_down, preferred_element_type=jnp.float32)
    shared_out = sent_and_summed(shared_part.astype(jnp.bfloat16), "tp", 1).astype(jnp.bfloat16)
    routed = moe(moe_rows, routes, route_scores, expert_gate, expert_up, expert_down)
    residual_half = lax.dynamic_slice_in_dim(residual, tp_index * half_width, half_width, 1)
    layer_out = (residual_half + routed + shared_out.astype(jnp.float32)).astype(jnp.bfloat16)
    return (layer_out, new_state)


def solution(mesh):
    return jax.shard_map(
        local,
        mesh=mesh,
        in_specs=(
            P("ep", None),
            P("ep", "tp", None, None),
            P(),
            P(),
            P(),
            P(None, "tp"),
            P(None, "tp"),
            P(None, "tp"),
            P(None, "tp"),
            P("tp"),
            P("tp", None),
            P("ep", None),
            P("ep", None),
            P("ep", None, "tp"),
            P("ep", None, "tp"),
            P("ep", "tp", None),
            P(None, "tp"),
            P(None, "tp"),
            P("tp", None),
        ),
        out_specs=(P("ep", "tp"), P("ep", "tp", None, None)),
        check_vma=False,
    )
```

```python
import functools

import jax
import jax.numpy as jnp
from jax import lax
from jax.experimental import pallas as pl
from jax.experimental.pallas import tpu as pltpu
from jax.sharding import PartitionSpec as P

epsilon = 1e-06
routed_scale = 2.5
MESH = pl.DeviceIdType.MESH
bf16, f32, i32 = jnp.bfloat16, jnp.float32, jnp.int32


def rms_scale(values, gain):
    return values * lax.rsqrt(jnp.mean(values * values, axis=-1, keepdims=True) + epsilon) * gain


def silu(v):
    return v / (1.0 + jnp.exp(-v))


def dot(a, b):
    return jnp.dot(a, b, preferred_element_type=f32)


def iota(shape, dim):
    return lax.broadcasted_iota(i32, shape, dim)


def toward(ep, off, sign):
    z, y, x = ep // 16, (ep // 4) % 4, ep % 4
    dz, dy, dx = off // 16, (off // 4) % 4, off % 4
    if sign < 0:
        dz, dy, dx = 4 - dz, 4 - dy, 4 - dx
    return ((z + dz) % 4) * 16 + ((y + dy) % 4) * 4 + (x + dx) % 4


def greet_all(ep, tp):
    barrier = pltpu.get_barrier_semaphore()

    def greet(i, c):
        peer = toward(ep, i, 1)
        for t in range(2):
            pl.semaphore_signal(barrier, inc=1, device_id=(peer, t), device_id_type=MESH)
        return c

    lax.fori_loop(1, 64, greet, 0)
    pl.semaphore_signal(barrier, inc=1, device_id=(ep, 1 - tp), device_id_type=MESH)


def await_all():
    pl.semaphore_wait(pltpu.get_barrier_semaphore(), 127)


def route_tables(routes, scores, ep):
    z, y, x = ep // 16, (ep // 4) % 4, ep % 4
    weights = scores / jnp.sum(scores, axis=0, keepdims=True) * routed_scale
    rz = ((routes >> 4) - z) & 3
    ry = (((routes >> 2) & 3) - y) & 3
    rx = ((routes & 3) - x) & 3
    rel = rz * 16 + ry * 4 + rx
    experts = iota((64, 16), 0)
    named = jnp.zeros((64, 16), f32)
    weight = jnp.zeros((64, 16), f32)
    for k in range(6):
        hit = rel[k : k + 1, :] == experts
        named = jnp.where(hit, 1.0, named)
        weight = jnp.where(hit, weights[k : k + 1, :], weight)
    earlier = (iota((16, 16), 0) < iota((16, 16), 1)).astype(bf16)
    rank = dot(named.astype(bf16), earlier)
    code = jnp.where(named > 0.5, rank + 1.0, 0.0)
    return code.astype(bf16), weight.astype(bf16)


def place_rows(code, tp, place_ref):
    spread = (iota((16, 128), 1) % 16 == iota((16, 128), 0)).astype(bf16)
    codes = dot(code, spread).astype(bf16)
    for b in range(4):
        grow = (iota((256, 64), 0) // 16 + 16 * b == iota((256, 64), 1)).astype(bf16)
        grown = dot(grow, codes)
        row = iota((256, 128), 0) % 16
        target = (2 * tp + row // 8 + 1).astype(f32)
        fits = (grown == target) & (iota((256, 128), 1) // 16 == row % 8)
        place_ref[pl.ds(256 * b, 256), :] = jnp.where(fits, 1.0, 0.0).astype(bf16)


def combine_rows(code, weight, comb_ref):
    both = jnp.concatenate([code, weight], axis=1)
    for n in range(8):
        col = iota((64, 256), 1) + 256 * n
        grow = (col // 32 == iota((64, 256), 0)).astype(bf16)
        grown = lax.dot_general(both, grow, (((0,), (0,)), ((), ())), preferred_element_type=f32)
        col = iota((16, 256), 1)
        slot = ((col // 8) % 4 + 1).astype(f32)
        value = jnp.where(grown[:16] == slot, grown[16:], 0.0)
        for j in range(8):
            comb_ref[pl.ds(16 * j, 16), pl.ds(256 * n, 256)] = jnp.where(
                col % 8 == j, value, 0.0
            ).astype(bf16)


def all_of(buf, n):
    return buf.at[pl.ds(0, n)]


def layer_kernel(
    tokens_hbm, state_hbm, mix_gain_hbm, moe_gain_hbm, head_gain_hbm, forget_hbm, query_hbm, input_hbm,
    outgate_hbm, bound_hbm, mix_out_hbm, routes_hbm, scores_hbm, gate_hbm, up_hbm, down_hbm,
    sgate_hbm, sup_hbm, sdown_hbm,
    out_ref, state_out,
    tokens_v, mix_gain_v, moe_gain_v, head_gain_v, bound_v, routes_v, scores_v,
    forget_w, query_w, input_w, outgate_w, state_v, mix_w, sgate_w, sup_w, sdown_w,
    gate_own, up_own, down_own, gate_par, up_par, down_par,
    mix_send, mix_recv, shared_send, shared_recv, residual_v,
    forget_t, key_t, input_h, place, comb, send, recv, xs, ret, back,
    load_sem, half_sem, state_sem, late_sem, push_sem, pull_sem, mix_sems, shared_sems, go_send, go_recv, ret_send, ret_recv,
):
    ep, tp = lax.axis_index("ep"), lax.axis_index("tp")
    partner = (ep, 1 - tp)

    def to_partner(src, dst, send_sem, recv_sem):
        return pltpu.make_async_remote_copy(
            src_ref=src, dst_ref=dst, send_sem=send_sem, recv_sem=recv_sem, device_id=partner, device_id_type=MESH
        )

    small = [
        pltpu.make_async_copy(src, dst, load_sem.at[i])
        for i, (src, dst) in enumerate(
            (
                (tokens_hbm, tokens_v), (mix_gain_hbm, mix_gain_v), (routes_hbm, routes_v), (scores_hbm, scores_v),
                (bound_hbm, bound_v), (head_gain_hbm, head_gain_v), (moe_gain_hbm, moe_gain_v),
            )
        )
    ]
    for copy in small:
        copy.start()
    halves = []
    for i, (src, dst) in enumerate(
        ((forget_hbm, forget_w), (query_hbm, query_w), (input_hbm, input_w), (outgate_hbm, outgate_w))
    ):
        for h in range(2):
            rows = pl.ds(1024 * h, 1024)
            halves.append(pltpu.make_async_copy(src.at[rows], dst.at[rows], half_sem.at[2 * i + h]))
            halves[-1].start()
    states = []
    for c in range(4):
        rows = pl.ds(4 * c, 4)
        states.append(pltpu.make_async_copy(state_hbm.at[rows], state_v.at[rows], state_sem.at[c]))
        states[-1].start()
    mix_load = pltpu.make_async_copy(mix_out_hbm, mix_w, late_sem.at[0])
    mix_load.start()
    greet_all(ep, tp)

    for copy in small:
        copy.wait()
    code, weight = route_tables(routes_v[...], scores_v[...], ep)
    tokens = tokens_v[...].astype(f32)
    normed = rms_scale(tokens, mix_gain_v[...]).astype(bf16)
    place_rows(code, tp, place)

    def project(i, w):
        halves[2 * i].wait()
        first = dot(normed[:, :1024], w[:1024])
        halves[2 * i + 1].wait()
        return first + dot(normed[:, 1024:], w[1024:])

    forget_pre = project(0, forget_w)
    bound = bound_v[...]
    forget = bound + (1.0 - bound) / (1.0 + jnp.exp(-forget_pre))
    key = (1.0 - bound) / (1.0 + jnp.exp(forget_pre))
    query = silu(project(1, query_w))
    seen = forget * query
    input_val = project(2, input_w)
    gate = silu(project(3, outgate_w))
    late = [
        pltpu.make_async_copy(src, dst, late_sem.at[1 + i])
        for i, (src, dst) in enumerate(
            (
                (sgate_hbm, sgate_w), (sup_hbm, sup_w), (sdown_hbm, sdown_w),
                (gate_hbm.at[0], gate_own), (up_hbm.at[0], up_own), (down_hbm.at[0], down_own),
            )
        )
    ]
    for copy in late:
        copy.start()
    heads = [slice(128 * h, 128 * h + 128) for h in range(4)]
    readout = [
        jnp.sum(key[:, at] * query[:, at], axis=-1, keepdims=True) * input_val[:, at] for at in heads
    ]
    row, block = iota((16, 512), 0), iota((16, 512), 1) // 128
    for c in range(4):
        states[c].wait()
        for h in range(4):
            tiled = jnp.concatenate([seen[:, heads[h]]] * 4, axis=1)
            spread = jnp.where(row == block + 4 * c, tiled, 0.0).astype(bf16)
            readout[h] += dot(spread, state_v[pl.ds(4 * c, 4), h].reshape(512, 128).astype(bf16))
    head_gain = head_gain_v[...]
    gated = jnp.concatenate(
        [rms_scale(readout[h], head_gain) * gate[:, heads[h]] for h in range(4)], axis=1
    ).astype(bf16)
    mix_load.wait()
    mix_send[...] = dot(gated, mix_w[...]).astype(bf16)
    await_all()
    mix_copy = to_partner(mix_send, mix_recv, mix_sems.at[0], mix_sems.at[1])
    mix_copy.start()
    pushes = [
        to_partner(src.at[0], dst, push_sem.at[i], pull_sem.at[i])
        for i, (src, dst) in enumerate(((gate_hbm, gate_par), (up_hbm, up_par), (down_hbm, down_par)))
    ]
    for copy in pushes:
        copy.start()
    mix_copy.wait()
    mixer = (mix_send[...].astype(f32) + mix_recv[...].astype(f32)).astype(bf16)
    residual = tokens + mixer.astype(f32)
    for h in range(2):
        residual_v[h] = residual[:, 1024 * h : 1024 * (h + 1)]
    rows = rms_scale(residual, moe_gain_v[...]).astype(bf16)
    stacked = jnp.concatenate([rows[:, 256 * j : 256 * (j + 1)] for j in range(8)], axis=0)

    def go(i):
        return pltpu.make_async_remote_copy(
            src_ref=send.at[i], dst_ref=recv.at[i], send_sem=go_send, recv_sem=go_recv,
            device_id=(toward(ep, i, 1), tp), device_id_type=MESH,
        )

    for b in range(4):
        placed = dot(place[pl.ds(256 * b, 256), :], stacked).astype(bf16)
        send[pl.ds(16 * b, 16)] = placed.reshape(16, 16, 256)

        def start(i, c):
            go(i).start()
            return c

        lax.fori_loop(max(1, 16 * b), 16 * b + 16, start, 0)
    recv[0] = send[0]

    for copy in late[:3]:
        copy.wait()
    shared_hidden = (silu(dot(rows, sgate_w[...])) * dot(rows, sup_w[...])).astype(bf16)
    shared_part = dot(shared_hidden, sdown_w[...]).astype(bf16)
    for h in range(2):
        shared_send[h] = shared_part[:, 1024 * h : 1024 * (h + 1)]
    shared_copy = to_partner(shared_send.at[1 - tp], shared_recv, shared_sems.at[0], shared_sems.at[1])
    shared_copy.start()
    combine_rows(code, weight, comb)
    for h in range(4):
        forget_t[h] = forget[:, heads[h]].T
        key_t[h] = key[:, heads[h]].T
        input_h[h] = input_val[:, heads[h]]

    def update(h, c):
        keep, add, value = forget_t[h], key_t[h], input_h[h]
        for s in range(16):
            state_out[s, h] = keep[:, s : s + 1] * state_v[s, h] + add[:, s : s + 1] * value[s : s + 1, :]
        return c

    lax.fori_loop(0, 4, update, 0)
    for copy in late[3:]:
        copy.wait()
    for copy in pushes:
        copy.wait()
    pltpu.make_async_remote_copy(
        src_ref=all_of(send, 63), dst_ref=all_of(recv, 63), send_sem=go_send, recv_sem=go_recv,
        device_id=partner, device_id_type=MESH,
    ).wait()

    out_row, in_row = iota((256, 256), 0), iota((256, 256), 1)
    sort = ((out_row // 32 == in_row % 8) & ((out_row // 2) % 16 == in_row // 16)
            & (out_row % 2 == (in_row // 8) % 2)).astype(bf16)
    unsort = ((in_row // 32 == out_row % 8) & ((in_row // 2) % 16 == out_row // 16)
              & (in_row % 2 == (out_row // 8) % 2)).astype(bf16)
    for b in range(4):
        sorted_rows = dot(sort, recv[pl.ds(16 * b, 16)].reshape(256, 256)).astype(bf16)
        for j in range(8):
            xs[pl.ds(32 * b, 32), pl.ds(256 * j, 256)] = sorted_rows[32 * j : 32 * j + 32]
    x = xs[...]
    hidden_own = (silu(dot(x, gate_own[...])) * dot(x, up_own[...])).astype(bf16)
    hidden_par = (silu(dot(x, gate_par[...])) * dot(x, up_par[...])).astype(bf16)
    for n in range(8):
        cols = pl.ds(256 * n, 256)
        xs[:, cols] = (dot(hidden_own, down_own[:, cols]) + dot(hidden_par, down_par[:, cols])).astype(bf16)

    def come(i, h):
        return pltpu.make_async_remote_copy(
            src_ref=ret.at[2 * i + h], dst_ref=back.at[2 * i + tp], send_sem=ret_send, recv_sem=ret_recv,
            device_id=(toward(ep, i, -1), h), device_id_type=MESH,
        )

    for b in range(4):
        tall = jnp.concatenate(
            [
                jnp.concatenate(
                    [xs[pl.ds(32 * b, 32), pl.ds(128 * j + 1024 * h, 128)] for h in range(2)], axis=1
                )
                for j in range(8)
            ],
            axis=0,
        )
        turned = dot(unsort, tall).astype(bf16)
        for i in range(16):
            for h in range(2):
                ret[2 * (16 * b + i) + h] = turned[16 * i : 16 * i + 16, 128 * h : 128 * h + 128]

        def start_back(i, c):
            for h in range(2):
                come(i, h).start()
            return c

        lax.fori_loop(max(1, 16 * b), 16 * b + 16, start_back, 0)
    to_partner(ret.at[1 - tp], back.at[tp], ret_send, ret_recv).start()
    back[tp] = ret[tp]
    shared_copy.wait()
    base = residual_v[tp] + (shared_send[tp].astype(f32) + shared_recv[...].astype(f32)).astype(bf16).astype(f32)
    to_partner(all_of(ret, 127), all_of(back, 127), ret_send, ret_recv).wait()
    total = dot(comb[...], back[...].reshape(2048, 128))
    for j in range(8):
        cols = slice(128 * j, 128 * (j + 1))
        out_ref[:, cols] = (base[:, cols] + total[16 * j : 16 * j + 16]).astype(bf16)


def local(
    tokens, state, mix_gain, moe_gain, head_gain, w_forget, w_query, w_input, w_outgate, lower_bound, w_mix_out,
    routes, route_scores, expert_gate, expert_up, expert_down, shared_gate, shared_up, shared_down,
):
    vm = pl.BlockSpec(memory_space=pltpu.VMEM)
    hbm = pl.BlockSpec(memory_space=pltpu.HBM)
    dma = pltpu.SemaphoreType.DMA

    def buf(*shape, dtype=bf16):
        return pltpu.VMEM(shape, dtype)

    return pl.pallas_call(
        layer_kernel,
        name="layer",
        out_shape=(jax.ShapeDtypeStruct((16, 1024), bf16), jax.ShapeDtypeStruct((16, 4, 128, 128), f32)),
        in_specs=[hbm] * 19,
        out_specs=(vm, vm),
        scratch_shapes=[
            buf(16, 2048), buf(1, 2048, dtype=f32), buf(1, 2048, dtype=f32), buf(1, 128, dtype=f32),
            buf(1, 512, dtype=f32), buf(6, 16, dtype=i32), buf(6, 16, dtype=f32),
            buf(2048, 512), buf(2048, 512), buf(2048, 512), buf(2048, 512), buf(16, 4, 128, 128, dtype=f32),
            buf(512, 2048), buf(2048, 256), buf(2048, 256), buf(256, 2048),
            buf(2048, 256), buf(2048, 256), buf(256, 2048), buf(2048, 256), buf(2048, 256), buf(256, 2048),
            buf(16, 2048), buf(16, 2048), buf(2, 16, 1024), buf(16, 1024), buf(2, 16, 1024, dtype=f32),
            buf(4, 128, 16, dtype=f32), buf(4, 128, 16, dtype=f32), buf(4, 16, 128, dtype=f32),
            buf(1024, 128), buf(128, 2048), buf(64, 16, 256), buf(64, 16, 256), buf(128, 2048),
            buf(128, 16, 128), buf(128, 16, 128),
            dma((7,)), dma((8,)), dma((4,)), dma((7,)), dma((3,)), dma((3,)), dma((2,)), dma((2,)), dma, dma, dma, dma,
        ],
        compiler_params=pltpu.CompilerParams(
            collective_id=0, has_side_effects=True, vmem_limit_bytes=56 << 20
        ),
    )(
        tokens, state, mix_gain.reshape(1, -1), moe_gain.reshape(1, -1), head_gain.reshape(1, -1),
        w_forget, w_query, w_input, w_outgate, lower_bound.reshape(1, -1), w_mix_out,
        routes.T, route_scores.T, expert_gate, expert_up, expert_down, shared_gate, shared_up, shared_down,
    )


def solution(mesh):
    return jax.shard_map(
        local,
        mesh=mesh,
        in_specs=(
            P("ep", None),
            P("ep", "tp", None, None),
            P(),
            P(),
            P(),
            P(None, "tp"),
            P(None, "tp"),
            P(None, "tp"),
            P(None, "tp"),
            P("tp"),
            P("tp", None),
            P("ep", None),
            P("ep", None),
            P("ep", None, "tp"),
            P("ep", None, "tp"),
            P("ep", "tp", None),
            P(None, "tp"),
            P(None, "tp"),
            P("tp", None),
        ),
        out_specs=(P("ep", "tp"), P("ep", "tp", None, None)),
        check_vma=False,
    )
```

```python
import functools

import jax
import jax.numpy as jnp
from jax import lax
from jax.experimental import pallas as pl
from jax.experimental.pallas import tpu as pltpu
from jax.sharding import PartitionSpec as P

epsilon = 1e-06
routed_scale = 2.5
MESH = pl.DeviceIdType.MESH
vmem_all = 67043328
bf16, f32, i32 = jnp.bfloat16, jnp.float32, jnp.int32


def rms_scale(values, gain):
    return values * lax.rsqrt(jnp.mean(values * values, axis=-1, keepdims=True) + epsilon) * gain


def silu(v):
    return v / (1.0 + jnp.exp(-v))


def dot(a, b):
    return jnp.dot(a, b, preferred_element_type=f32)


def iota(shape, dim):
    return lax.broadcasted_iota(i32, shape, dim)


def toward(ep, off, sign):
    z, y, x = ep // 16, (ep // 4) % 4, ep % 4
    dz, dy, dx = off // 16, (off // 4) % 4, off % 4
    if sign < 0:
        dz, dy, dx = 4 - dz, 4 - dy, 4 - dx
    return ((z + dz) % 4) * 16 + ((y + dy) % 4) * 4 + (x + dx) % 4


def greet_all(ep, tp):
    barrier = pltpu.get_barrier_semaphore()

    def greet(i, c):
        peer = toward(ep, i, 1)
        for t in range(2):
            pl.semaphore_signal(barrier, inc=1, device_id=(peer, t), device_id_type=MESH)
        return c

    lax.fori_loop(1, 64, greet, 0)
    pl.semaphore_signal(barrier, inc=1, device_id=(ep, 1 - tp), device_id_type=MESH)


def await_all():
    pl.semaphore_wait(pltpu.get_barrier_semaphore(), 127)


def route_tables(routes, scores, ep):
    z, y, x = ep // 16, (ep // 4) % 4, ep % 4
    weights = scores / jnp.sum(scores, axis=0, keepdims=True) * routed_scale
    rz = ((routes >> 4) - z) & 3
    ry = (((routes >> 2) & 3) - y) & 3
    rx = ((routes & 3) - x) & 3
    rel = rz * 16 + ry * 4 + rx
    experts = iota((64, 16), 0)
    named = jnp.zeros((64, 16), f32)
    weight = jnp.zeros((64, 16), f32)
    for k in range(6):
        hit = rel[k : k + 1, :] == experts
        named = jnp.where(hit, 1.0, named)
        weight = jnp.where(hit, weights[k : k + 1, :], weight)
    earlier = (iota((16, 16), 0) < iota((16, 16), 1)).astype(bf16)
    rank = dot(named.astype(bf16), earlier)
    code = jnp.where(named > 0.5, rank + 1.0, 0.0)
    return code.astype(bf16), weight.astype(bf16)


def place_rows(code, tp, place_ref):
    spread = (iota((16, 128), 1) % 16 == iota((16, 128), 0)).astype(bf16)
    codes = dot(code, spread).astype(bf16)
    for b in range(4):
        grow = (iota((256, 64), 0) // 16 + 16 * b == iota((256, 64), 1)).astype(bf16)
        grown = dot(grow, codes)
        row = iota((256, 128), 0) % 16
        target = (2 * tp + row // 8 + 1).astype(f32)
        fits = (grown == target) & (iota((256, 128), 1) // 16 == row % 8)
        place_ref[pl.ds(256 * b, 256), :] = jnp.where(fits, 1.0, 0.0).astype(bf16)


def combine_rows(code, weight, comb_ref):
    both = jnp.concatenate([code, weight], axis=1)
    for n in range(8):
        col = iota((64, 256), 1) + 256 * n
        grow = (col // 32 == iota((64, 256), 0)).astype(bf16)
        grown = lax.dot_general(both, grow, (((0,), (0,)), ((), ())), preferred_element_type=f32)
        col = iota((16, 256), 1)
        slot = ((col // 8) % 4 + 1).astype(f32)
        value = jnp.where(grown[:16] == slot, grown[16:], 0.0)
        for j in range(8):
            comb_ref[pl.ds(16 * j, 16), pl.ds(256 * n, 256)] = jnp.where(
                col % 8 == j, value, 0.0
            ).astype(bf16)


def all_of(buf, n):
    return buf.at[pl.ds(0, n)]


def layer_kernel(
    tokens_hbm, state_hbm, mix_gain_hbm, moe_gain_hbm, head_gain_hbm, forget_hbm, query_hbm, input_hbm,
    outgate_hbm, bound_hbm, mix_out_hbm, routes_hbm, scores_hbm, gate_hbm, up_hbm, down_hbm,
    sgate_hbm, sup_hbm, sdown_hbm,
    state_out, back, comb, base_out,
    tokens_v, mix_gain_v, moe_gain_v, head_gain_v, bound_v, routes_v, scores_v,
    forget_w, query_w, input_w, outgate_w, state_v, mix_w, sgate_w, sup_w, sdown_w,
    gate_own, up_own, down_own, gate_par, up_par, down_par,
    mix_send, mix_recv, shared_send, shared_recv, residual_v,
    forget_t, key_t, input_h, place, send, recv, xs, ret,
    load_sem, half_sem, state_sem, late_sem, push_sem, pull_sem, mix_sems, shared_sems, go_send, go_recv, ret_send, ret_recv,
):
    ep, tp = lax.axis_index("ep"), lax.axis_index("tp")
    partner = (ep, 1 - tp)

    def to_partner(src, dst, send_sem, recv_sem):
        return pltpu.make_async_remote_copy(
            src_ref=src, dst_ref=dst, send_sem=send_sem, recv_sem=recv_sem, device_id=partner, device_id_type=MESH
        )

    small = [
        pltpu.make_async_copy(src, dst, load_sem.at[i])
        for i, (src, dst) in enumerate(
            (
                (tokens_hbm, tokens_v), (mix_gain_hbm, mix_gain_v), (routes_hbm, routes_v), (scores_hbm, scores_v),
                (bound_hbm, bound_v), (head_gain_hbm, head_gain_v), (moe_gain_hbm, moe_gain_v),
            )
        )
    ]
    for copy in small:
        copy.start()
    halves = []
    for i, (src, dst) in enumerate(
        ((forget_hbm, forget_w), (query_hbm, query_w), (input_hbm, input_w), (outgate_hbm, outgate_w))
    ):
        for h in range(2):
            rows = pl.ds(1024 * h, 1024)
            halves.append(pltpu.make_async_copy(src.at[rows], dst.at[rows], half_sem.at[2 * i + h]))
            halves[-1].start()
    states = []
    for c in range(4):
        rows = pl.ds(4 * c, 4)
        states.append(pltpu.make_async_copy(state_hbm.at[rows], state_v.at[rows], state_sem.at[c]))
        states[-1].start()
    mix_load = pltpu.make_async_copy(mix_out_hbm, mix_w, late_sem.at[0])
    mix_load.start()
    greet_all(ep, tp)

    for copy in small:
        copy.wait()
    code, weight = route_tables(routes_v[...], scores_v[...], ep)
    tokens = tokens_v[...].astype(f32)
    normed = rms_scale(tokens, mix_gain_v[...]).astype(bf16)
    place_rows(code, tp, place)

    def project(i, w):
        halves[2 * i].wait()
        first = dot(normed[:, :1024], w[:1024])
        halves[2 * i + 1].wait()
        return first + dot(normed[:, 1024:], w[1024:])

    forget_pre = project(0, forget_w)
    bound = bound_v[...]
    forget = bound + (1.0 - bound) / (1.0 + jnp.exp(-forget_pre))
    key = (1.0 - bound) / (1.0 + jnp.exp(forget_pre))
    query = silu(project(1, query_w))
    seen = forget * query
    input_val = project(2, input_w)
    gate = silu(project(3, outgate_w))
    late = [
        pltpu.make_async_copy(src, dst, late_sem.at[1 + i])
        for i, (src, dst) in enumerate(
            (
                (sgate_hbm, sgate_w), (sup_hbm, sup_w), (sdown_hbm, sdown_w),
                (gate_hbm.at[0], gate_own), (up_hbm.at[0], up_own), (down_hbm.at[0], down_own),
            )
        )
    ]
    for copy in late:
        copy.start()
    heads = [slice(128 * h, 128 * h + 128) for h in range(4)]
    readout = [
        jnp.sum(key[:, at] * query[:, at], axis=-1, keepdims=True) * input_val[:, at] for at in heads
    ]
    row, block = iota((16, 512), 0), iota((16, 512), 1) // 128
    for c in range(4):
        states[c].wait()
        for h in range(4):
            tiled = jnp.concatenate([seen[:, heads[h]]] * 4, axis=1)
            spread = jnp.where(row == block + 4 * c, tiled, 0.0).astype(bf16)
            readout[h] += dot(spread, state_v[pl.ds(4 * c, 4), h].reshape(512, 128).astype(bf16))
    head_gain = head_gain_v[...]
    gated = jnp.concatenate(
        [rms_scale(readout[h], head_gain) * gate[:, heads[h]] for h in range(4)], axis=1
    ).astype(bf16)
    mix_load.wait()
    mix_send[...] = dot(gated, mix_w[...]).astype(bf16)
    await_all()
    mix_copy = to_partner(mix_send, mix_recv, mix_sems.at[0], mix_sems.at[1])
    mix_copy.start()
    pushes = [
        to_partner(src.at[0], dst, push_sem.at[i], pull_sem.at[i])
        for i, (src, dst) in enumerate(((gate_hbm, gate_par), (up_hbm, up_par), (down_hbm, down_par)))
    ]
    for copy in pushes:
        copy.start()
    mix_copy.wait()
    mixer = (mix_send[...].astype(f32) + mix_recv[...].astype(f32)).astype(bf16)
    residual = tokens + mixer.astype(f32)
    for h in range(2):
        residual_v[h] = residual[:, 1024 * h : 1024 * (h + 1)]
    rows = rms_scale(residual, moe_gain_v[...]).astype(bf16)
    stacked = jnp.concatenate([rows[:, 256 * j : 256 * (j + 1)] for j in range(8)], axis=0)

    def go(i):
        return pltpu.make_async_remote_copy(
            src_ref=send.at[i], dst_ref=recv.at[i], send_sem=go_send, recv_sem=go_recv,
            device_id=(toward(ep, i, 1), tp), device_id_type=MESH,
        )

    for b in range(4):
        placed = dot(place[pl.ds(256 * b, 256), :], stacked).astype(bf16)
        send[pl.ds(16 * b, 16)] = placed.reshape(16, 16, 256)

        def start(i, c):
            go(i).start()
            return c

        lax.fori_loop(max(1, 16 * b), 16 * b + 16, start, 0)
    recv[0] = send[0]

    for copy in late[:3]:
        copy.wait()
    shared_hidden = (silu(dot(rows, sgate_w[...])) * dot(rows, sup_w[...])).astype(bf16)
    shared_part = dot(shared_hidden, sdown_w[...]).astype(bf16)
    for h in range(2):
        shared_send[h] = shared_part[:, 1024 * h : 1024 * (h + 1)]
    shared_copy = to_partner(shared_send.at[1 - tp], shared_recv, shared_sems.at[0], shared_sems.at[1])
    shared_copy.start()
    combine_rows(code, weight, comb)
    for h in range(4):
        forget_t[h] = forget[:, heads[h]].T
        key_t[h] = key[:, heads[h]].T
        input_h[h] = input_val[:, heads[h]]

    def update(h, c):
        keep, add, value = forget_t[h], key_t[h], input_h[h]
        for s in range(16):
            state_out[s, h] = keep[:, s : s + 1] * state_v[s, h] + add[:, s : s + 1] * value[s : s + 1, :]
        return c

    lax.fori_loop(0, 4, update, 0)
    for copy in late[3:]:
        copy.wait()
    for copy in pushes:
        copy.wait()
    pltpu.make_async_remote_copy(
        src_ref=all_of(send, 63), dst_ref=all_of(recv, 63), send_sem=go_send, recv_sem=go_recv,
        device_id=partner, device_id_type=MESH,
    ).wait()

    out_row, in_row = iota((256, 256), 0), iota((256, 256), 1)
    sort = ((out_row // 32 == in_row % 8) & ((out_row // 2) % 16 == in_row // 16)
            & (out_row % 2 == (in_row // 8) % 2)).astype(bf16)
    unsort = ((in_row // 32 == out_row % 8) & ((in_row // 2) % 16 == out_row // 16)
              & (in_row % 2 == (out_row // 8) % 2)).astype(bf16)
    for b in range(4):
        sorted_rows = dot(sort, recv[pl.ds(16 * b, 16)].reshape(256, 256)).astype(bf16)
        for j in range(8):
            xs[pl.ds(32 * b, 32), pl.ds(256 * j, 256)] = sorted_rows[32 * j : 32 * j + 32]
    x = xs[...]
    hidden_own = (silu(dot(x, gate_own[...])) * dot(x, up_own[...])).astype(bf16)
    hidden_par = (silu(dot(x, gate_par[...])) * dot(x, up_par[...])).astype(bf16)
    for n in range(8):
        cols = pl.ds(256 * n, 256)
        xs[:, cols] = (dot(hidden_own, down_own[:, cols]) + dot(hidden_par, down_par[:, cols])).astype(bf16)

    def come(i, h):
        return pltpu.make_async_remote_copy(
            src_ref=ret.at[2 * i + h], dst_ref=back.at[2 * i + tp], send_sem=ret_send, recv_sem=ret_recv,
            device_id=(toward(ep, i, -1), h), device_id_type=MESH,
        )

    for b in range(4):
        tall = jnp.concatenate(
            [
                jnp.concatenate(
                    [xs[pl.ds(32 * b, 32), pl.ds(128 * j + 1024 * h, 128)] for h in range(2)], axis=1
                )
                for j in range(8)
            ],
            axis=0,
        )
        turned = dot(unsort, tall).astype(bf16)
        for i in range(16):
            for h in range(2):
                ret[2 * (16 * b + i) + h] = turned[16 * i : 16 * i + 16, 128 * h : 128 * h + 128]

        def start_back(i, c):
            for h in range(2):
                come(i, h).start()
            return c

        lax.fori_loop(max(1, 16 * b), 16 * b + 16, start_back, 0)
    to_partner(ret.at[1 - tp], back.at[tp], ret_send, ret_recv).start()
    back[tp] = ret[tp]
    shared_copy.wait()
    base_out[...] = residual_v[tp] + (shared_send[tp].astype(f32) + shared_recv[...].astype(f32)).astype(bf16).astype(f32)
    to_partner(all_of(ret, 127), all_of(back, 127), ret_send, ret_recv).wait()


def finish_kernel(state_ref, back_ref, comb_ref, base_ref, out_hbm, state_hbm, out_v, sems):
    state_copy = pltpu.make_async_copy(state_ref, state_hbm, sems.at[0])
    state_copy.start()
    total = dot(comb_ref[...], back_ref[...].reshape(2048, 128))
    for j in range(8):
        cols = slice(128 * j, 128 * (j + 1))
        out_v[:, cols] = (base_ref[:, cols] + total[16 * j : 16 * j + 16]).astype(bf16)
    out_copy = pltpu.make_async_copy(out_v, out_hbm, sems.at[1])
    out_copy.start()
    out_copy.wait()
    state_copy.wait()


def local(
    tokens, state, mix_gain, moe_gain, head_gain, w_forget, w_query, w_input, w_outgate, lower_bound, w_mix_out,
    routes, route_scores, expert_gate, expert_up, expert_down, shared_gate, shared_up, shared_down,
):
    vm = pl.BlockSpec(memory_space=pltpu.VMEM)
    hbm = pl.BlockSpec(memory_space=pltpu.HBM)
    dma = pltpu.SemaphoreType.DMA

    def buf(*shape, dtype=bf16):
        return pltpu.VMEM(shape, dtype)

    kept = pl.pallas_call(
        layer_kernel,
        name="layer",
        out_shape=(
            buf(16, 4, 128, 128, dtype=f32), buf(128, 16, 128), buf(128, 2048), buf(16, 1024, dtype=f32)
        ),
        in_specs=[hbm] * 19,
        out_specs=(vm,) * 4,
        scratch_shapes=[
            buf(16, 2048), buf(1, 2048, dtype=f32), buf(1, 2048, dtype=f32), buf(1, 128, dtype=f32),
            buf(1, 512, dtype=f32), buf(6, 16, dtype=i32), buf(6, 16, dtype=f32),
            buf(2048, 512), buf(2048, 512), buf(2048, 512), buf(2048, 512), buf(16, 4, 128, 128, dtype=f32),
            buf(512, 2048), buf(2048, 256), buf(2048, 256), buf(256, 2048),
            buf(2048, 256), buf(2048, 256), buf(256, 2048), buf(2048, 256), buf(2048, 256), buf(256, 2048),
            buf(16, 2048), buf(16, 2048), buf(2, 16, 1024), buf(16, 1024), buf(2, 16, 1024, dtype=f32),
            buf(4, 128, 16, dtype=f32), buf(4, 128, 16, dtype=f32), buf(4, 16, 128, dtype=f32),
            buf(1024, 128), buf(64, 16, 256), buf(64, 16, 256), buf(128, 2048), buf(128, 16, 128),
            dma((7,)), dma((8,)), dma((4,)), dma((7,)), dma((3,)), dma((3,)), dma((2,)), dma((2,)), dma, dma, dma, dma,
        ],
        compiler_params=pltpu.CompilerParams(
            collective_id=0, has_side_effects=True, vmem_limit_bytes=vmem_all - (5 << 20) - (160 << 10)
        ),
    )(
        tokens, state, mix_gain.reshape(1, -1), moe_gain.reshape(1, -1), head_gain.reshape(1, -1),
        w_forget, w_query, w_input, w_outgate, lower_bound.reshape(1, -1), w_mix_out,
        routes.T, route_scores.T, expert_gate, expert_up, expert_down, shared_gate, shared_up, shared_down,
    )
    return pl.pallas_call(
        finish_kernel,
        name="finish",
        out_shape=(jax.ShapeDtypeStruct((16, 1024), bf16), jax.ShapeDtypeStruct((16, 4, 128, 128), f32)),
        in_specs=[vm] * 4,
        out_specs=(hbm, hbm),
        scratch_shapes=[buf(16, 1024), dma((2,))],
        compiler_params=pltpu.CompilerParams(vmem_limit_bytes=8 << 20),
    )(*kept)


def solution(mesh):
    return jax.shard_map(
        local,
        mesh=mesh,
        in_specs=(
            P("ep", None),
            P("ep", "tp", None, None),
            P(),
            P(),
            P(),
            P(None, "tp"),
            P(None, "tp"),
            P(None, "tp"),
            P(None, "tp"),
            P("tp"),
            P("tp", None),
            P("ep", None),
            P("ep", None),
            P("ep", None, "tp"),
            P("ep", None, "tp"),
            P("ep", "tp", None),
            P(None, "tp"),
            P(None, "tp"),
            P("tp", None),
        ),
        out_specs=(P("ep", "tp"), P("ep", "tp", None, None)),
        check_vma=False,
    )
```

```python
import jax
import jax.numpy as jnp
import numpy as np
from jax import lax
from jax.experimental import pallas as pl
from jax.experimental.pallas import tpu as pltpu
from jax.sharding import PartitionSpec as P

epsilon = 1e-06
routed_scale = 2.5
MESH = pl.DeviceIdType.MESH
vmem_all = 67043328
bf16, f32, i32 = jnp.bfloat16, jnp.float32, jnp.int32


def rms_scale(values, gain):
    return values * lax.rsqrt(jnp.mean(values * values, axis=-1, keepdims=True) + epsilon) * gain


def silu(v):
    return v / (1.0 + jnp.exp(-v))


def dot(a, b):
    return jnp.dot(a, b, preferred_element_type=f32)


def iota(shape, dim):
    return lax.broadcasted_iota(i32, shape, dim)


def parts(off):
    return off // 16, off // 4 % 4, off % 4


def hops(off):
    return sum(min(d, 4 - d) for d in parts(off))


order = sorted(range(64), key=lambda off: (-hops(off), off * 37 % 64))


class Peers:
    def __init__(self, ep):
        z, y, x = ep // 16, lax.rem(ep // 4, 4), lax.rem(ep, 4)
        self.z = [lax.rem(z + d, 4) * 16 for d in range(4)]
        self.y = [lax.rem(y + d, 4) * 4 for d in range(4)]
        self.x = [lax.rem(x + d, 4) for d in range(4)]

    def ahead(self, p):
        dz, dy, dx = parts(order[p])
        return self.z[dz] + self.y[dy] + self.x[dx]

    def behind(self, p):
        dz, dy, dx = parts(order[p])
        return self.z[-dz % 4] + self.y[-dy % 4] + self.x[-dx % 4]


def greet_all(ep, tp, peers):
    barrier = pltpu.get_barrier_semaphore()
    for p in range(63):
        for t in range(2):
            pl.semaphore_signal(barrier, inc=1, device_id=(peers.ahead(p), t), device_id_type=MESH)
    pl.semaphore_signal(barrier, inc=1, device_id=(ep, 1 - tp), device_id_type=MESH)


def await_all():
    pl.semaphore_wait(pltpu.get_barrier_semaphore(), 127)


def route_tables(routes, scores, experts, ep):
    z, y, x = ep // 16, (ep // 4) % 4, ep % 4
    weights = scores / jnp.sum(scores, axis=0, keepdims=True) * routed_scale
    rz = ((routes >> 4) - z) & 3
    ry = (((routes >> 2) & 3) - y) & 3
    rx = ((routes & 3) - x) & 3
    rel = rz * 16 + ry * 4 + rx
    named = jnp.zeros((64, 16), f32)
    weight = jnp.zeros((64, 16), f32)
    for k in range(6):
        hit = rel[k : k + 1, :] == experts
        named = jnp.where(hit, 1.0, named)
        weight = jnp.where(hit, weights[k : k + 1, :], weight)
    earlier = (iota((16, 16), 0) < iota((16, 16), 1)).astype(bf16)
    rank = dot(named.astype(bf16), earlier)
    code = jnp.where(named > 0.5, rank + 1.0, 0.0)
    return code.astype(bf16), weight.astype(bf16)


def place_rows(code, tp, place_ref):
    spread = (iota((16, 128), 1) % 16 == iota((16, 128), 0)).astype(bf16)
    codes = dot(code, spread).astype(bf16)
    for b in range(4):
        grow = (iota((256, 64), 0) // 16 + 16 * b == iota((256, 64), 1)).astype(bf16)
        grown = dot(grow, codes)
        row = iota((256, 128), 0) % 16
        target = (2 * tp + row // 8 + 1).astype(f32)
        fits = (grown == target) & (iota((256, 128), 1) // 16 == row % 8)
        place_ref[pl.ds(256 * b, 256), :] = jnp.where(fits, 1.0, 0.0).astype(bf16)


def combine_rows(code, weight, comb_ref):
    both = jnp.concatenate([code, weight], axis=1)
    for n in range(8):
        col = iota((64, 256), 1) + 256 * n
        grow = (col // 32 == iota((64, 256), 0)).astype(bf16)
        grown = lax.dot_general(both, grow, (((0,), (0,)), ((), ())), preferred_element_type=f32)
        col = iota((16, 256), 1)
        slot = ((col // 8) % 4 + 1).astype(f32)
        value = jnp.where(grown[:16] == slot, grown[16:], 0.0)
        for j in range(8):
            comb_ref[pl.ds(16 * j, 16), pl.ds(256 * n, 256)] = jnp.where(
                col % 8 == j, value, 0.0
            ).astype(bf16)


def all_of(buf, n):
    return buf.at[pl.ds(0, n)]


def layer_kernel(
    tokens_hbm, state_hbm, mix_gain_hbm, moe_gain_hbm, head_gain_hbm, forget_hbm, query_hbm, input_hbm,
    outgate_hbm, bound_hbm, mix_out_hbm, routes_hbm, scores_hbm, gate_hbm, up_hbm, down_hbm,
    sgate_hbm, sup_hbm, sdown_hbm, order_hbm,
    state_out, back, comb, base_out,
    tokens_v, mix_gain_v, moe_gain_v, head_gain_v, bound_v, routes_v, scores_v, order_v,
    forget_w, query_w, input_w, outgate_w, state_v, mix_w, sgate_w, sup_w, sdown_w,
    gate_own, up_own, down_own, gate_par, up_par, down_par,
    mix_send, mix_recv, shared_send, shared_recv, residual_v,
    forget_t, key_t, input_h, place, send, recv, xs, ret,
    load_sem, half_sem, state_sem, late_sem, push_sem, pull_sem, mix_sems, shared_sems, go_send, go_recv, ret_send, ret_recv,
):
    ep, tp = lax.axis_index("ep"), lax.axis_index("tp")
    partner = (ep, 1 - tp)

    def to_partner(src, dst, send_sem, recv_sem):
        return pltpu.make_async_remote_copy(
            src_ref=src, dst_ref=dst, send_sem=send_sem, recv_sem=recv_sem, device_id=partner, device_id_type=MESH
        )

    small = [
        pltpu.make_async_copy(src, dst, load_sem.at[i])
        for i, (src, dst) in enumerate(
            (
                (tokens_hbm, tokens_v), (mix_gain_hbm, mix_gain_v), (bound_hbm, bound_v), (routes_hbm, routes_v),
                (scores_hbm, scores_v), (head_gain_hbm, head_gain_v), (moe_gain_hbm, moe_gain_v), (order_hbm, order_v),
            )
        )
    ]
    for copy in small:
        copy.start()
    halves = []
    for i, (src, dst) in enumerate(
        ((forget_hbm, forget_w), (query_hbm, query_w), (input_hbm, input_w), (outgate_hbm, outgate_w))
    ):
        for h in range(2):
            rows = pl.ds(1024 * h, 1024)
            halves.append(pltpu.make_async_copy(src.at[rows], dst.at[rows], half_sem.at[2 * i + h]))
            halves[-1].start()
    states = []
    for c in range(4):
        rows = pl.ds(4 * c, 4)
        states.append(pltpu.make_async_copy(state_hbm.at[rows], state_v.at[rows], state_sem.at[c]))
        states[-1].start()
    mix_load = pltpu.make_async_copy(mix_out_hbm, mix_w, late_sem.at[0])
    mix_load.start()
    peers = Peers(ep)
    greet_all(ep, tp, peers)

    for copy in small[:2]:
        copy.wait()
    tokens = tokens_v[...].astype(f32)
    normed = rms_scale(tokens, mix_gain_v[...]).astype(bf16)

    def project(i, w):
        halves[2 * i].wait()
        first = dot(normed[:, :1024], w[:1024])
        halves[2 * i + 1].wait()
        return first + dot(normed[:, 1024:], w[1024:])

    forget_pre = project(0, forget_w)
    small[2].wait()
    bound = bound_v[...]
    forget = bound + (1.0 - bound) / (1.0 + jnp.exp(-forget_pre))
    key = (1.0 - bound) / (1.0 + jnp.exp(forget_pre))
    query = silu(project(1, query_w))
    seen = forget * query
    input_val = project(2, input_w)
    gate = silu(project(3, outgate_w))
    heads = [slice(128 * h, 128 * h + 128) for h in range(4)]
    readout = [
        jnp.sum(key[:, at] * query[:, at], axis=-1, keepdims=True) * input_val[:, at] for at in heads
    ]
    row, block = iota((16, 512), 0), iota((16, 512), 1) // 128
    for c in range(4):
        states[c].wait()
        for h in range(4):
            tiled = jnp.concatenate([seen[:, heads[h]]] * 4, axis=1)
            spread = jnp.where(row == block + 4 * c, tiled, 0.0).astype(bf16)
            readout[h] += dot(spread, state_v[pl.ds(4 * c, 4), h].reshape(512, 128).astype(bf16))
    for copy in small[3:]:
        copy.wait()
    head_gain = head_gain_v[...]
    gated = jnp.concatenate(
        [rms_scale(readout[h], head_gain) * gate[:, heads[h]] for h in range(4)], axis=1
    ).astype(bf16)
    late = [
        pltpu.make_async_copy(src, dst, late_sem.at[1 + i])
        for i, (src, dst) in enumerate(
            (
                (sgate_hbm, sgate_w), (sup_hbm, sup_w), (sdown_hbm, sdown_w),
                (gate_hbm.at[0], gate_own), (up_hbm.at[0], up_own), (down_hbm.at[0], down_own),
            )
        )
    ]
    for copy in late:
        copy.start()
    mix_load.wait()
    mix_send[...] = dot(gated, mix_w[...]).astype(bf16)
    await_all()
    mix_copy = to_partner(mix_send, mix_recv, mix_sems.at[0], mix_sems.at[1])
    mix_copy.start()
    pushes = [
        to_partner(src.at[0], dst, push_sem.at[i], pull_sem.at[i])
        for i, (src, dst) in enumerate(((gate_hbm, gate_par), (up_hbm, up_par), (down_hbm, down_par)))
    ]
    for copy in pushes:
        copy.start()
    code, weight = route_tables(routes_v[...], scores_v[...], order_v[...], ep)
    place_rows(code, tp, place)
    mix_copy.wait()
    mixer = (mix_send[...].astype(f32) + mix_recv[...].astype(f32)).astype(bf16)
    residual = tokens + mixer.astype(f32)
    for h in range(2):
        residual_v[h] = residual[:, 1024 * h : 1024 * (h + 1)]
    rows = rms_scale(residual, moe_gain_v[...]).astype(bf16)
    stacked = jnp.concatenate([rows[:, 256 * j : 256 * (j + 1)] for j in range(8)], axis=0)

    for b in range(4):
        placed = dot(place[pl.ds(256 * b, 256), :], stacked).astype(bf16)
        send[pl.ds(16 * b, 16)] = placed.reshape(16, 16, 256)
        for p in range(16 * b, min(16 * b + 16, 63)):
            pltpu.make_async_remote_copy(
                src_ref=send.at[p], dst_ref=recv.at[p], send_sem=go_send, recv_sem=go_recv.at[p // 32],
                device_id=(peers.ahead(p), tp), device_id_type=MESH,
            ).start()
    recv[63] = send[63]

    for copy in late[:3]:
        copy.wait()
    shared_hidden = (silu(dot(rows, sgate_w[...])) * dot(rows, sup_w[...])).astype(bf16)
    shared_part = dot(shared_hidden, sdown_w[...]).astype(bf16)
    for h in range(2):
        shared_send[h] = shared_part[:, 1024 * h : 1024 * (h + 1)]
    shared_copy = to_partner(shared_send.at[1 - tp], shared_recv, shared_sems.at[0], shared_sems.at[1])
    shared_copy.start()
    combine_rows(code, weight, comb)
    for h in range(4):
        forget_t[h] = forget[:, heads[h]].T
        key_t[h] = key[:, heads[h]].T
        input_h[h] = input_val[:, heads[h]]

    def update(h, c):
        keep, add, value = forget_t[h], key_t[h], input_h[h]
        for s in range(16):
            state_out[s, h] = keep[:, s : s + 1] * state_v[s, h] + add[:, s : s + 1] * value[s : s + 1, :]
        return c

    lax.fori_loop(0, 4, update, 0)
    out_row, in_row = iota((256, 256), 0), iota((256, 256), 1)
    sort = ((out_row // 32 == in_row % 8) & ((out_row // 2) % 16 == in_row // 16)
            & (out_row % 2 == (in_row // 8) % 2)).astype(bf16)
    unsort = ((in_row // 32 == out_row % 8) & ((in_row // 2) % 16 == out_row // 16)
              & (in_row % 2 == (out_row // 8) % 2)).astype(bf16)
    for copy in late[3:]:
        copy.wait()
    for g in range(2):
        group = pl.ds(32 * g, 32 - g)
        to_partner(send.at[group], recv.at[group], go_send, go_recv.at[g]).wait_recv()
        for b in range(2):
            sorted_rows = dot(sort, recv[pl.ds(32 * g + 16 * b, 16)].reshape(256, 256)).astype(bf16)
            for j in range(8):
                xs[g, pl.ds(32 * b, 32), pl.ds(256 * j, 256)] = sorted_rows[32 * j : 32 * j + 32]
        x = xs[g]
        hidden_own = (silu(dot(x, gate_own[...])) * dot(x, up_own[...])).astype(bf16)
        if g == 0:
            for copy in pushes:
                copy.wait()
        hidden_par = (silu(dot(x, gate_par[...])) * dot(x, up_par[...])).astype(bf16)
        for n in range(8):
            cols = pl.ds(256 * n, 256)
            xs[g, :, cols] = (dot(hidden_own, down_own[:, cols]) + dot(hidden_par, down_par[:, cols])).astype(bf16)
        for b in range(2):
            tall = jnp.concatenate(
                [
                    jnp.concatenate(
                        [xs[g, pl.ds(32 * b, 32), pl.ds(128 * j + 1024 * h, 128)] for h in range(2)], axis=1
                    )
                    for j in range(8)
                ],
                axis=0,
            )
            turned = dot(unsort, tall).astype(bf16)
            for i in range(16):
                p = 32 * g + 16 * b + i
                for h in range(2):
                    ret[2 * p + h] = turned[16 * i : 16 * i + 16, 128 * h : 128 * h + 128]
                    if p < 63:
                        pltpu.make_async_remote_copy(
                            src_ref=ret.at[2 * p + h], dst_ref=back.at[2 * p + tp], send_sem=ret_send,
                            recv_sem=ret_recv, device_id=(peers.behind(p), h), device_id_type=MESH,
                        ).start()
    to_partner(ret.at[127 - tp], back.at[126 + tp], ret_send, ret_recv).start()
    back[126 + tp] = ret[126 + tp]
    shared_copy.wait()
    base_out[...] = residual_v[tp] + (shared_send[tp].astype(f32) + shared_recv[...].astype(f32)).astype(bf16).astype(f32)
    to_partner(all_of(send, 63), all_of(recv, 63), go_send, go_recv.at[0]).wait_send()
    to_partner(all_of(ret, 127), all_of(back, 127), ret_send, ret_recv).wait()


def finish_kernel(state_ref, back_ref, comb_ref, base_ref, out_hbm, state_hbm, out_v, sems):
    state_copy = pltpu.make_async_copy(state_ref, state_hbm, sems.at[0])
    state_copy.start()
    total = dot(comb_ref[...], back_ref[...].reshape(2048, 128))
    for j in range(8):
        cols = slice(128 * j, 128 * (j + 1))
        out_v[:, cols] = (base_ref[:, cols] + total[16 * j : 16 * j + 16]).astype(bf16)
    out_copy = pltpu.make_async_copy(out_v, out_hbm, sems.at[1])
    out_copy.start()
    out_copy.wait()
    state_copy.wait()


def local(
    tokens, state, mix_gain, moe_gain, head_gain, w_forget, w_query, w_input, w_outgate, lower_bound, w_mix_out,
    routes, route_scores, expert_gate, expert_up, expert_down, shared_gate, shared_up, shared_down,
):
    vm = pl.BlockSpec(memory_space=pltpu.VMEM)
    hbm = pl.BlockSpec(memory_space=pltpu.HBM)
    dma = pltpu.SemaphoreType.DMA

    def buf(*shape, dtype=bf16):
        return pltpu.VMEM(shape, dtype)

    kept = pl.pallas_call(
        layer_kernel,
        name="layer",
        out_shape=(
            buf(16, 4, 128, 128, dtype=f32), buf(128, 16, 128), buf(128, 2048), buf(16, 1024, dtype=f32)
        ),
        in_specs=[hbm] * 20,
        out_specs=(vm,) * 4,
        scratch_shapes=[
            buf(16, 2048), buf(1, 2048, dtype=f32), buf(1, 2048, dtype=f32), buf(1, 128, dtype=f32),
            buf(1, 512, dtype=f32), buf(6, 16, dtype=i32), buf(6, 16, dtype=f32), buf(64, 16, dtype=i32),
            buf(2048, 512), buf(2048, 512), buf(2048, 512), buf(2048, 512), buf(16, 4, 128, 128, dtype=f32),
            buf(512, 2048), buf(2048, 256), buf(2048, 256), buf(256, 2048),
            buf(2048, 256), buf(2048, 256), buf(256, 2048), buf(2048, 256), buf(2048, 256), buf(256, 2048),
            buf(16, 2048), buf(16, 2048), buf(2, 16, 1024), buf(16, 1024), buf(2, 16, 1024, dtype=f32),
            buf(4, 128, 16, dtype=f32), buf(4, 128, 16, dtype=f32), buf(4, 16, 128, dtype=f32),
            buf(1024, 128), buf(64, 16, 256), buf(64, 16, 256), buf(2, 64, 2048), buf(128, 16, 128),
            dma((8,)), dma((8,)), dma((4,)), dma((7,)), dma((3,)), dma((3,)), dma((2,)), dma((2,)), dma, dma((2,)), dma, dma,
        ],
        compiler_params=pltpu.CompilerParams(
            collective_id=0, has_side_effects=True, vmem_limit_bytes=vmem_all - (5 << 20) - (160 << 10)
        ),
    )(
        tokens, state, mix_gain.reshape(1, -1), moe_gain.reshape(1, -1), head_gain.reshape(1, -1),
        w_forget, w_query, w_input, w_outgate, lower_bound.reshape(1, -1), w_mix_out,
        routes.T, route_scores.T, expert_gate, expert_up, expert_down, shared_gate, shared_up, shared_down,
        jnp.asarray(np.repeat(np.array(order, np.int32)[:, None], 16, 1)),
    )
    return pl.pallas_call(
        finish_kernel,
        name="finish",
        out_shape=(jax.ShapeDtypeStruct((16, 1024), bf16), jax.ShapeDtypeStruct((16, 4, 128, 128), f32)),
        in_specs=[vm] * 4,
        out_specs=(hbm, hbm),
        scratch_shapes=[buf(16, 1024), dma((2,))],
        compiler_params=pltpu.CompilerParams(vmem_limit_bytes=8 << 20),
    )(*kept)


def solution(mesh):
    return jax.shard_map(
        local,
        mesh=mesh,
        in_specs=(
            P("ep", None),
            P("ep", "tp", None, None),
            P(),
            P(),
            P(),
            P(None, "tp"),
            P(None, "tp"),
            P(None, "tp"),
            P(None, "tp"),
            P("tp"),
            P("tp", None),
            P("ep", None),
            P("ep", None),
            P("ep", None, "tp"),
            P("ep", None, "tp"),
            P("ep", "tp", None),
            P(None, "tp"),
            P(None, "tp"),
            P("tp", None),
        ),
        out_specs=(P("ep", "tp"), P("ep", "tp", None, None)),
        check_vma=False,
    )
```

```python
import jax
import jax.numpy as jnp
import numpy as np
from jax import lax
from jax.experimental import pallas as pl
from jax.experimental.pallas import tpu as pltpu
from jax.sharding import PartitionSpec as P

epsilon = 1e-06
routed_scale = 2.5
MESH = pl.DeviceIdType.MESH
vmem_all = 67043328
bf16, f32, i32 = jnp.bfloat16, jnp.float32, jnp.int32


def rms_scale(values, gain):
    return values * lax.rsqrt(jnp.mean(values * values, axis=-1, keepdims=True) + epsilon) * gain


def silu(v):
    return v / (1.0 + jnp.exp(-v))


def dot(a, b):
    return jnp.dot(a, b, preferred_element_type=f32)


def iota(shape, dim):
    return lax.broadcasted_iota(i32, shape, dim)


def parts(off):
    return off // 16, off // 4 % 4, off % 4


def hops(off):
    return sum(min(d, 4 - d) for d in parts(off))


order = sorted(range(64), key=lambda off: (-hops(off), off * 37 % 64))


class Peers:
    def __init__(self, ep):
        z, y, x = ep // 16, lax.rem(ep // 4, 4), lax.rem(ep, 4)
        self.z = [lax.rem(z + d, 4) * 16 for d in range(4)]
        self.y = [lax.rem(y + d, 4) * 4 for d in range(4)]
        self.x = [lax.rem(x + d, 4) for d in range(4)]

    def ahead(self, p):
        dz, dy, dx = parts(order[p])
        return self.z[dz] + self.y[dy] + self.x[dx]

    def behind(self, p):
        dz, dy, dx = parts(order[p])
        return self.z[-dz % 4] + self.y[-dy % 4] + self.x[-dx % 4]


def greet_all(ep, tp, peers):
    barrier = pltpu.get_barrier_semaphore()
    for p in range(63):
        for t in range(2):
            pl.semaphore_signal(barrier, inc=1, device_id=(peers.ahead(p), t), device_id_type=MESH)
    pl.semaphore_signal(barrier, inc=1, device_id=(ep, 1 - tp), device_id_type=MESH)


def await_all():
    pl.semaphore_wait(pltpu.get_barrier_semaphore(), 127)


def route_tables(routes, scores, experts, ep):
    z, y, x = ep // 16, (ep // 4) % 4, ep % 4
    weights = scores / jnp.sum(scores, axis=0, keepdims=True) * routed_scale
    rz = ((routes >> 4) - z) & 3
    ry = (((routes >> 2) & 3) - y) & 3
    rx = ((routes & 3) - x) & 3
    rel = rz * 16 + ry * 4 + rx
    named = jnp.zeros((64, 16), f32)
    weight = jnp.zeros((64, 16), f32)
    for k in range(6):
        hit = rel[k : k + 1, :] == experts
        named = jnp.where(hit, 1.0, named)
        weight = jnp.where(hit, weights[k : k + 1, :], weight)
    earlier = (iota((16, 16), 0) < iota((16, 16), 1)).astype(bf16)
    rank = dot(named.astype(bf16), earlier)
    code = jnp.where(named > 0.5, rank + 1.0, 0.0)
    return code.astype(bf16), weight.astype(bf16)


def place_rows(code, tp, place_ref):
    spread = (iota((16, 128), 1) % 16 == iota((16, 128), 0)).astype(bf16)
    codes = dot(code, spread).astype(bf16)
    for b in range(4):
        grow = (iota((256, 64), 0) // 16 + 16 * b == iota((256, 64), 1)).astype(bf16)
        grown = dot(grow, codes)
        row = iota((256, 128), 0) % 16
        target = (2 * tp + row // 8 + 1).astype(f32)
        fits = (grown == target) & (iota((256, 128), 1) // 16 == row % 8)
        place_ref[pl.ds(256 * b, 256), :] = jnp.where(fits, 1.0, 0.0).astype(bf16)


def combine_rows(code, weight, comb_ref):
    both = jnp.concatenate([code, weight], axis=1)
    for n in range(8):
        col = iota((64, 256), 1) + 256 * n
        grow = (col // 32 == iota((64, 256), 0)).astype(bf16)
        grown = lax.dot_general(both, grow, (((0,), (0,)), ((), ())), preferred_element_type=f32)
        col = iota((16, 256), 1)
        slot = ((col // 8) % 4 + 1).astype(f32)
        value = jnp.where(grown[:16] == slot, grown[16:], 0.0)
        for j in range(8):
            comb_ref[pl.ds(16 * j, 16), pl.ds(256 * n, 256)] = jnp.where(
                col % 8 == j, value, 0.0
            ).astype(bf16)


def all_of(buf, n):
    return buf.at[pl.ds(0, n)]


def layer_kernel(
    tokens_hbm, state_hbm, mix_gain_hbm, moe_gain_hbm, head_gain_hbm, forget_hbm, query_hbm, input_hbm,
    outgate_hbm, bound_hbm, mix_out_hbm, routes_hbm, scores_hbm, gate_hbm, up_hbm, down_hbm,
    sgate_hbm, sup_hbm, sdown_hbm, order_hbm,
    state_out, back, comb, base_out,
    tokens_v, mix_gain_v, moe_gain_v, head_gain_v, bound_v, routes_v, scores_v, order_v,
    forget_w, query_w, input_w, outgate_w, state_v, mix_w, sgate_w, sup_w, sdown_w,
    gate_own, up_own, down_own, gate_par, up_par, down_par,
    mix_send, mix_recv, shared_send, shared_recv, residual_v,
    forget_t, key_t, input_h, place, send, recv, xs, ret,
    load_sem, half_sem, state_sem, mix_load_sem, late_sem, push_sem, pull_sem, mix_sems, shared_sems, go_send, go_recv, ret_send, ret_recv,
):
    ep, tp = lax.axis_index("ep"), lax.axis_index("tp")
    partner = (ep, 1 - tp)

    def to_partner(src, dst, send_sem, recv_sem):
        return pltpu.make_async_remote_copy(
            src_ref=src, dst_ref=dst, send_sem=send_sem, recv_sem=recv_sem, device_id=partner, device_id_type=MESH
        )

    small = [
        pltpu.make_async_copy(src, dst, load_sem.at[i])
        for i, (src, dst) in enumerate(
            (
                (tokens_hbm, tokens_v), (mix_gain_hbm, mix_gain_v), (bound_hbm, bound_v), (routes_hbm, routes_v),
                (scores_hbm, scores_v), (head_gain_hbm, head_gain_v), (moe_gain_hbm, moe_gain_v), (order_hbm, order_v),
            )
        )
    ]
    for copy in small:
        copy.start()
    big = []
    for i, (src, dst) in enumerate(
        (
            (forget_hbm, forget_w), (query_hbm, query_w), (input_hbm, input_w), (outgate_hbm, outgate_w)
        )
    ):
        for h in range(2):
            rows = pl.ds(1024 * h, 1024)
            big.append(pltpu.make_async_copy(src.at[rows], dst.at[rows], half_sem.at[2 * i + h]))
    for c in range(4):
        rows = pl.ds(4 * c, 4)
        big.append(pltpu.make_async_copy(state_hbm.at[rows], state_v.at[rows], state_sem.at[c]))
    for h in range(2):
        cols = pl.ds(1024 * h, 1024)
        big.append(pltpu.make_async_copy(mix_out_hbm.at[:, cols], mix_w.at[:, cols], mix_load_sem.at[h]))
    ahead = 8
    for copy in big[:ahead]:
        copy.start()

    def take(i):
        big[i].wait()
        if i + ahead < len(big):
            big[i + ahead].start()

    peers = Peers(ep)
    greet_all(ep, tp, peers)

    for copy in small[:2]:
        copy.wait()
    tokens = tokens_v[...].astype(f32)
    normed = rms_scale(tokens, mix_gain_v[...]).astype(bf16)

    def project(i, w):
        take(2 * i)
        first = dot(normed[:, :1024], w[:1024])
        take(2 * i + 1)
        return first + dot(normed[:, 1024:], w[1024:])

    forget_pre = project(0, forget_w)
    small[2].wait()
    bound = bound_v[...]
    forget = bound + (1.0 - bound) / (1.0 + jnp.exp(-forget_pre))
    key = (1.0 - bound) / (1.0 + jnp.exp(forget_pre))
    query = silu(project(1, query_w))
    seen = forget * query
    input_val = project(2, input_w)
    gate = silu(project(3, outgate_w))
    heads = [slice(128 * h, 128 * h + 128) for h in range(4)]
    readout = [
        jnp.sum(key[:, at] * query[:, at], axis=-1, keepdims=True) * input_val[:, at] for at in heads
    ]
    row, block = iota((16, 512), 0), iota((16, 512), 1) // 128
    for c in range(4):
        take(8 + c)
        for h in range(4):
            tiled = jnp.concatenate([seen[:, heads[h]]] * 4, axis=1)
            spread = jnp.where(row == block + 4 * c, tiled, 0.0).astype(bf16)
            readout[h] += dot(spread, state_v[pl.ds(4 * c, 4), h].reshape(512, 128).astype(bf16))
    for copy in small[3:]:
        copy.wait()
    head_gain = head_gain_v[...]
    gated = jnp.concatenate(
        [rms_scale(readout[h], head_gain) * gate[:, heads[h]] for h in range(4)], axis=1
    ).astype(bf16)
    for h in range(2):
        cols = pl.ds(1024 * h, 1024)
        take(12 + h)
        mix_send[:, cols] = dot(gated, mix_w[:, cols]).astype(bf16)
    late = [
        pltpu.make_async_copy(src, dst, late_sem.at[i])
        for i, (src, dst) in enumerate(
            (
                (sgate_hbm, sgate_w), (sup_hbm, sup_w), (sdown_hbm, sdown_w),
                (gate_hbm.at[0], gate_own), (up_hbm.at[0], up_own), (down_hbm.at[0], down_own),
            )
        )
    ]
    for copy in late:
        copy.start()
    await_all()
    mix_copy = to_partner(mix_send, mix_recv, mix_sems.at[0], mix_sems.at[1])
    mix_copy.start()
    pushes = [
        to_partner(src.at[0], dst, push_sem.at[i], pull_sem.at[i])
        for i, (src, dst) in enumerate(((gate_hbm, gate_par), (up_hbm, up_par), (down_hbm, down_par)))
    ]
    for copy in pushes:
        copy.start()
    code, weight = route_tables(routes_v[...], scores_v[...], order_v[...], ep)
    place_rows(code, tp, place)
    mix_copy.wait()
    mixer = (mix_send[...].astype(f32) + mix_recv[...].astype(f32)).astype(bf16)
    residual = tokens + mixer.astype(f32)
    for h in range(2):
        residual_v[h] = residual[:, 1024 * h : 1024 * (h + 1)]
    rows = rms_scale(residual, moe_gain_v[...]).astype(bf16)
    stacked = jnp.concatenate([rows[:, 256 * j : 256 * (j + 1)] for j in range(8)], axis=0)

    for b in range(4):
        placed = dot(place[pl.ds(256 * b, 256), :], stacked).astype(bf16)
        send[pl.ds(16 * b, 16)] = placed.reshape(16, 16, 256)
    for p in list(range(16, 63)) + list(range(16)):
        pltpu.make_async_remote_copy(
            src_ref=send.at[p], dst_ref=recv.at[p], send_sem=go_send, recv_sem=go_recv.at[int(p >= 16)],
            device_id=(peers.ahead(p), tp), device_id_type=MESH,
        ).start()
    recv[63] = send[63]

    for copy in late[:3]:
        copy.wait()
    shared_hidden = (silu(dot(rows, sgate_w[...])) * dot(rows, sup_w[...])).astype(bf16)
    shared_part = dot(shared_hidden, sdown_w[...]).astype(bf16)
    for h in range(2):
        shared_send[h] = shared_part[:, 1024 * h : 1024 * (h + 1)]
    shared_copy = to_partner(shared_send.at[1 - tp], shared_recv, shared_sems.at[0], shared_sems.at[1])
    shared_copy.start()
    combine_rows(code, weight, comb)
    for h in range(4):
        forget_t[h] = forget[:, heads[h]].T
        key_t[h] = key[:, heads[h]].T
        input_h[h] = input_val[:, heads[h]]

    def update(h, c):
        keep, add, value = forget_t[h], key_t[h], input_h[h]
        for s in range(16):
            state_out[s, h] = keep[:, s : s + 1] * state_v[s, h] + add[:, s : s + 1] * value[s : s + 1, :]
        return c

    lax.fori_loop(0, 4, update, 0)
    out_row, in_row = iota((256, 256), 0), iota((256, 256), 1)
    sort = ((out_row // 32 == in_row % 8) & ((out_row // 2) % 16 == in_row // 16)
            & (out_row % 2 == (in_row // 8) % 2)).astype(bf16)
    unsort = ((in_row // 32 == out_row % 8) & ((in_row // 2) % 16 == out_row // 16)
              & (in_row % 2 == (out_row // 8) % 2)).astype(bf16)
    for copy in late[3:]:
        copy.wait()
    for g, blocks in ((1, range(1, 4)), (0, range(1))):
        group = pl.ds(16 * blocks[0], 16 * len(blocks) - g)
        mine = pl.ds(32 * blocks[0], 32 * len(blocks))
        to_partner(send.at[group], recv.at[group], go_send, go_recv.at[g]).wait_recv()
        for b in blocks:
            sorted_rows = dot(sort, recv[pl.ds(16 * b, 16)].reshape(256, 256)).astype(bf16)
            for j in range(8):
                xs[pl.ds(32 * b, 32), pl.ds(256 * j, 256)] = sorted_rows[32 * j : 32 * j + 32]
        x = xs[mine, :]
        hidden_own = (silu(dot(x, gate_own[...])) * dot(x, up_own[...])).astype(bf16)
        if g == 1:
            for copy in pushes:
                copy.wait()
        hidden_par = (silu(dot(x, gate_par[...])) * dot(x, up_par[...])).astype(bf16)
        for n in range(8):
            cols = pl.ds(256 * n, 256)
            xs[mine, cols] = (dot(hidden_own, down_own[:, cols]) + dot(hidden_par, down_par[:, cols])).astype(bf16)
        for b in blocks:
            tall = jnp.concatenate(
                [
                    jnp.concatenate(
                        [xs[pl.ds(32 * b, 32), pl.ds(128 * j + 1024 * h, 128)] for h in range(2)], axis=1
                    )
                    for j in range(8)
                ],
                axis=0,
            )
            turned = dot(unsort, tall).astype(bf16)
            for i in range(16):
                p = 16 * b + i
                for h in range(2):
                    ret[2 * p + h] = turned[16 * i : 16 * i + 16, 128 * h : 128 * h + 128]
                    if p < 63:
                        pltpu.make_async_remote_copy(
                            src_ref=ret.at[2 * p + h], dst_ref=back.at[2 * p + tp], send_sem=ret_send,
                            recv_sem=ret_recv, device_id=(peers.behind(p), h), device_id_type=MESH,
                        ).start()
    to_partner(ret.at[127 - tp], back.at[126 + tp], ret_send, ret_recv).start()
    back[126 + tp] = ret[126 + tp]
    shared_copy.wait()
    base_out[...] = residual_v[tp] + (shared_send[tp].astype(f32) + shared_recv[...].astype(f32)).astype(bf16).astype(f32)
    to_partner(all_of(send, 63), all_of(recv, 63), go_send, go_recv.at[0]).wait_send()
    to_partner(all_of(ret, 127), all_of(back, 127), ret_send, ret_recv).wait()


def finish_kernel(state_ref, back_ref, comb_ref, base_ref, out_hbm, state_hbm, out_v, sems):
    state_copy = pltpu.make_async_copy(state_ref, state_hbm, sems.at[0])
    state_copy.start()
    total = dot(comb_ref[...], back_ref[...].reshape(2048, 128))
    for j in range(8):
        cols = slice(128 * j, 128 * (j + 1))
        out_v[:, cols] = (base_ref[:, cols] + total[16 * j : 16 * j + 16]).astype(bf16)
    out_copy = pltpu.make_async_copy(out_v, out_hbm, sems.at[1])
    out_copy.start()
    out_copy.wait()
    state_copy.wait()


def local(
    tokens, state, mix_gain, moe_gain, head_gain, w_forget, w_query, w_input, w_outgate, lower_bound, w_mix_out,
    routes, route_scores, expert_gate, expert_up, expert_down, shared_gate, shared_up, shared_down,
):
    vm = pl.BlockSpec(memory_space=pltpu.VMEM)
    hbm = pl.BlockSpec(memory_space=pltpu.HBM)
    dma = pltpu.SemaphoreType.DMA

    def buf(*shape, dtype=bf16):
        return pltpu.VMEM(shape, dtype)

    kept = pl.pallas_call(
        layer_kernel,
        name="layer",
        out_shape=(
            buf(16, 4, 128, 128, dtype=f32), buf(128, 16, 128), buf(128, 2048), buf(16, 1024, dtype=f32)
        ),
        in_specs=[hbm] * 20,
        out_specs=(vm,) * 4,
        scratch_shapes=[
            buf(16, 2048), buf(1, 2048, dtype=f32), buf(1, 2048, dtype=f32), buf(1, 128, dtype=f32),
            buf(1, 512, dtype=f32), buf(6, 16, dtype=i32), buf(6, 16, dtype=f32), buf(64, 16, dtype=i32),
            buf(2048, 512), buf(2048, 512), buf(2048, 512), buf(2048, 512), buf(16, 4, 128, 128, dtype=f32),
            buf(512, 2048), buf(2048, 256), buf(2048, 256), buf(256, 2048),
            buf(2048, 256), buf(2048, 256), buf(256, 2048), buf(2048, 256), buf(2048, 256), buf(256, 2048),
            buf(16, 2048), buf(16, 2048), buf(2, 16, 1024), buf(16, 1024), buf(2, 16, 1024, dtype=f32),
            buf(4, 128, 16, dtype=f32), buf(4, 128, 16, dtype=f32), buf(4, 16, 128, dtype=f32),
            buf(1024, 128), buf(64, 16, 256), buf(64, 16, 256), buf(128, 2048), buf(128, 16, 128),
            dma((8,)), dma((8,)), dma((4,)), dma((2,)), dma((6,)), dma((3,)), dma((3,)), dma((2,)), dma((2,)), dma, dma((2,)), dma, dma,
        ],
        compiler_params=pltpu.CompilerParams(
            collective_id=0, has_side_effects=True, vmem_limit_bytes=vmem_all - (5 << 20) - (160 << 10)
        ),
    )(
        tokens, state, mix_gain.reshape(1, -1), moe_gain.reshape(1, -1), head_gain.reshape(1, -1),
        w_forget, w_query, w_input, w_outgate, lower_bound.reshape(1, -1), w_mix_out,
        routes.T, route_scores.T, expert_gate, expert_up, expert_down, shared_gate, shared_up, shared_down,
        jnp.asarray(np.repeat(np.array(order, np.int32)[:, None], 16, 1)),
    )
    return pl.pallas_call(
        finish_kernel,
        name="finish",
        out_shape=(jax.ShapeDtypeStruct((16, 1024), bf16), jax.ShapeDtypeStruct((16, 4, 128, 128), f32)),
        in_specs=[vm] * 4,
        out_specs=(hbm, hbm),
        scratch_shapes=[buf(16, 1024), dma((2,))],
        compiler_params=pltpu.CompilerParams(vmem_limit_bytes=8 << 20),
    )(*kept)


def solution(mesh):
    return jax.shard_map(
        local,
        mesh=mesh,
        in_specs=(
            P("ep", None),
            P("ep", "tp", None, None),
            P(),
            P(),
            P(),
            P(None, "tp"),
            P(None, "tp"),
            P(None, "tp"),
            P(None, "tp"),
            P("tp"),
            P("tp", None),
            P("ep", None),
            P("ep", None),
            P("ep", None, "tp"),
            P("ep", None, "tp"),
            P("ep", "tp", None),
            P(None, "tp"),
            P(None, "tp"),
            P("tp", None),
        ),
        out_specs=(P("ep", "tp"), P("ep", "tp", None, None)),
        check_vma=False,
    )
```

```python
import jax
import jax.numpy as jnp
import numpy as np
from jax import lax
from jax.experimental import pallas as pl
from jax.experimental.pallas import tpu as pltpu
from jax.sharding import PartitionSpec as P

epsilon = 1e-06
routed_scale = 2.5
MESH = pl.DeviceIdType.MESH
vmem_all = 67043328
bf16, f32, i32 = jnp.bfloat16, jnp.float32, jnp.int32


def rms_scale(values, gain):
    return values * lax.rsqrt(jnp.mean(values * values, axis=-1, keepdims=True) + epsilon) * gain


def silu(v):
    return v / (1.0 + jnp.exp(-v))


def dot(a, b):
    return jnp.dot(a, b, preferred_element_type=f32)


def iota(shape, dim):
    return lax.broadcasted_iota(i32, shape, dim)


def parts(off):
    return off // 16, off // 4 % 4, off % 4


def hops(off):
    return sum(min(d, 4 - d) for d in parts(off))


def turns(off):
    return sum(d > 0 for d in parts(off))


order = sorted(range(64), key=lambda off: (-hops(off), -turns(off), off * 37 % 64))


class Peers:
    def __init__(self, ep):
        z, y, x = ep // 16, lax.rem(ep // 4, 4), lax.rem(ep, 4)
        self.z = [lax.rem(z + d, 4) * 16 for d in range(4)]
        self.y = [lax.rem(y + d, 4) * 4 for d in range(4)]
        self.x = [lax.rem(x + d, 4) for d in range(4)]

    def ahead(self, p):
        dz, dy, dx = parts(order[p])
        return self.z[dz] + self.y[dy] + self.x[dx]

    def behind(self, p):
        dz, dy, dx = parts(order[p])
        return self.z[-dz % 4] + self.y[-dy % 4] + self.x[-dx % 4]


def greet_all(ep, tp, peers):
    barrier = pltpu.get_barrier_semaphore()
    for p in range(63):
        for t in range(2):
            pl.semaphore_signal(barrier, inc=1, device_id=(peers.ahead(p), t), device_id_type=MESH)
    pl.semaphore_signal(barrier, inc=1, device_id=(ep, 1 - tp), device_id_type=MESH)


def await_all():
    pl.semaphore_wait(pltpu.get_barrier_semaphore(), 127)


def route_tables(routes, scores, experts, ep):
    z, y, x = ep // 16, (ep // 4) % 4, ep % 4
    weights = scores / jnp.sum(scores, axis=0, keepdims=True) * routed_scale
    rz = ((routes >> 4) - z) & 3
    ry = (((routes >> 2) & 3) - y) & 3
    rx = ((routes & 3) - x) & 3
    rel = rz * 16 + ry * 4 + rx
    named = jnp.zeros((64, 16), f32)
    weight = jnp.zeros((64, 16), f32)
    for k in range(6):
        hit = rel[k : k + 1, :] == experts
        named = jnp.where(hit, 1.0, named)
        weight = jnp.where(hit, weights[k : k + 1, :], weight)
    earlier = (iota((16, 16), 0) < iota((16, 16), 1)).astype(bf16)
    rank = dot(named.astype(bf16), earlier)
    code = jnp.where(named > 0.5, rank + 1.0, 0.0)
    return code.astype(bf16), weight.astype(bf16)


def place_rows(code, tp, place_ref):
    spread = (iota((16, 128), 1) % 16 == iota((16, 128), 0)).astype(bf16)
    codes = dot(code, spread).astype(bf16)
    for b in range(4):
        grow = (iota((256, 64), 0) // 16 + 16 * b == iota((256, 64), 1)).astype(bf16)
        grown = dot(grow, codes)
        row = iota((256, 128), 0) % 16
        target = (2 * tp + row // 8 + 1).astype(f32)
        fits = (grown == target) & (iota((256, 128), 1) // 16 == row % 8)
        place_ref[pl.ds(256 * b, 256), :] = jnp.where(fits, 1.0, 0.0).astype(bf16)


def combine_rows(code, weight, comb_ref):
    both = jnp.concatenate([code, weight], axis=1)
    for n in range(8):
        col = iota((64, 256), 1) + 256 * n
        grow = (col // 32 == iota((64, 256), 0)).astype(bf16)
        grown = lax.dot_general(both, grow, (((0,), (0,)), ((), ())), preferred_element_type=f32)
        col = iota((16, 256), 1)
        slot = ((col // 8) % 4 + 1).astype(f32)
        value = jnp.where(grown[:16] == slot, grown[16:], 0.0)
        for j in range(8):
            comb_ref[pl.ds(16 * j, 16), pl.ds(256 * n, 256)] = jnp.where(
                col % 8 == j, value, 0.0
            ).astype(bf16)


def all_of(buf, n):
    return buf.at[pl.ds(0, n)]


def layer_kernel(
    tokens_hbm, state_hbm, mix_gain_hbm, moe_gain_hbm, head_gain_hbm, forget_hbm, query_hbm, input_hbm,
    outgate_hbm, bound_hbm, mix_out_hbm, routes_hbm, scores_hbm, gate_hbm, up_hbm, down_hbm,
    sgate_hbm, sup_hbm, sdown_hbm, order_hbm,
    state_out, back, comb, base_out,
    tokens_v, mix_gain_v, moe_gain_v, head_gain_v, bound_v, routes_v, scores_v, order_v,
    forget_w, query_w, input_w, outgate_w, state_v, mix_w, sgate_w, sup_w, sdown_w,
    gate_own, up_own, down_own, gate_par, up_par, down_par,
    mix_send, mix_recv, shared_send, shared_recv, residual_v,
    forget_t, key_t, input_h, place, send, recv, xs, ret,
    load_sem, half_sem, state_sem, mix_load_sem, late_sem, push_sem, pull_sem, mix_sems, shared_sems, go_send, go_recv, ret_send, ret_recv,
):
    ep, tp = lax.axis_index("ep"), lax.axis_index("tp")
    partner = (ep, 1 - tp)

    def to_partner(src, dst, send_sem, recv_sem):
        return pltpu.make_async_remote_copy(
            src_ref=src, dst_ref=dst, send_sem=send_sem, recv_sem=recv_sem, device_id=partner, device_id_type=MESH
        )

    small = [
        pltpu.make_async_copy(src, dst, load_sem.at[i])
        for i, (src, dst) in enumerate(
            (
                (tokens_hbm, tokens_v), (mix_gain_hbm, mix_gain_v), (bound_hbm, bound_v), (routes_hbm, routes_v),
                (scores_hbm, scores_v), (head_gain_hbm, head_gain_v), (moe_gain_hbm, moe_gain_v), (order_hbm, order_v),
            )
        )
    ]
    for copy in small:
        copy.start()
    big = []
    for i, (src, dst) in enumerate(
        (
            (forget_hbm, forget_w), (query_hbm, query_w), (input_hbm, input_w), (outgate_hbm, outgate_w)
        )
    ):
        for h in range(2):
            rows = pl.ds(1024 * h, 1024)
            big.append(pltpu.make_async_copy(src.at[rows], dst.at[rows], half_sem.at[2 * i + h]))
    for c in range(4):
        rows = pl.ds(4 * c, 4)
        big.append(pltpu.make_async_copy(state_hbm.at[rows], state_v.at[rows], state_sem.at[c]))
    for h in range(2):
        cols = pl.ds(1024 * h, 1024)
        big.append(pltpu.make_async_copy(mix_out_hbm.at[:, cols], mix_w.at[:, cols], mix_load_sem.at[h]))
    ahead = 8
    for copy in big[:ahead]:
        copy.start()

    def take(i):
        big[i].wait()
        if i + ahead < len(big):
            big[i + ahead].start()

    peers = Peers(ep)
    greet_all(ep, tp, peers)

    for copy in small[:2]:
        copy.wait()
    tokens = tokens_v[...].astype(f32)
    normed = rms_scale(tokens, mix_gain_v[...]).astype(bf16)

    def project(i, w):
        take(2 * i)
        first = dot(normed[:, :1024], w[:1024])
        take(2 * i + 1)
        return first + dot(normed[:, 1024:], w[1024:])

    forget_pre = project(0, forget_w)
    small[2].wait()
    bound = bound_v[...]
    forget = bound + (1.0 - bound) / (1.0 + jnp.exp(-forget_pre))
    key = (1.0 - bound) / (1.0 + jnp.exp(forget_pre))
    query = silu(project(1, query_w))
    seen = forget * query
    input_val = project(2, input_w)
    gate = silu(project(3, outgate_w))
    heads = [slice(128 * h, 128 * h + 128) for h in range(4)]
    readout = [
        jnp.sum(key[:, at] * query[:, at], axis=-1, keepdims=True) * input_val[:, at] for at in heads
    ]
    row, block = iota((16, 512), 0), iota((16, 512), 1) // 128
    for c in range(4):
        take(8 + c)
        for h in range(4):
            tiled = jnp.concatenate([seen[:, heads[h]]] * 4, axis=1)
            spread = jnp.where(row == block + 4 * c, tiled, 0.0).astype(bf16)
            readout[h] += dot(spread, state_v[pl.ds(4 * c, 4), h].reshape(512, 128).astype(bf16))
    for copy in small[3:]:
        copy.wait()
    head_gain = head_gain_v[...]
    gated = jnp.concatenate(
        [rms_scale(readout[h], head_gain) * gate[:, heads[h]] for h in range(4)], axis=1
    ).astype(bf16)
    for h in range(2):
        cols = pl.ds(1024 * h, 1024)
        take(12 + h)
        mix_send[:, cols] = dot(gated, mix_w[:, cols]).astype(bf16)
    late = [
        pltpu.make_async_copy(src, dst, late_sem.at[i])
        for i, (src, dst) in enumerate(
            (
                (sgate_hbm, sgate_w), (sup_hbm, sup_w), (sdown_hbm, sdown_w),
                (gate_hbm.at[0], gate_own), (up_hbm.at[0], up_own), (down_hbm.at[0], down_own),
            )
        )
    ]
    for copy in late:
        copy.start()
    await_all()
    mix_copy = to_partner(mix_send, mix_recv, mix_sems.at[0], mix_sems.at[1])
    mix_copy.start()
    pushes = [
        to_partner(src.at[0], dst, push_sem.at[i], pull_sem.at[i])
        for i, (src, dst) in enumerate(((gate_hbm, gate_par), (up_hbm, up_par), (down_hbm, down_par)))
    ]
    for copy in pushes:
        copy.start()
    code, weight = route_tables(routes_v[...], scores_v[...], order_v[...], ep)
    place_rows(code, tp, place)
    mix_copy.wait()
    mixer = (mix_send[...].astype(f32) + mix_recv[...].astype(f32)).astype(bf16)
    residual = tokens + mixer.astype(f32)
    for h in range(2):
        residual_v[h] = residual[:, 1024 * h : 1024 * (h + 1)]
    rows = rms_scale(residual, moe_gain_v[...]).astype(bf16)
    stacked = jnp.concatenate([rows[:, 256 * j : 256 * (j + 1)] for j in range(8)], axis=0)

    for b in range(4):
        placed = dot(place[pl.ds(256 * b, 256), :], stacked).astype(bf16)
        send[pl.ds(16 * b, 16)] = placed.reshape(16, 16, 256)
    for p in list(range(16, 63)) + list(range(16)):
        pltpu.make_async_remote_copy(
            src_ref=send.at[p], dst_ref=recv.at[p], send_sem=go_send, recv_sem=go_recv.at[int(p >= 16)],
            device_id=(peers.ahead(p), tp), device_id_type=MESH,
        ).start()
    recv[63] = send[63]

    for copy in late[:3]:
        copy.wait()
    shared_hidden = (silu(dot(rows, sgate_w[...])) * dot(rows, sup_w[...])).astype(bf16)
    shared_part = dot(shared_hidden, sdown_w[...]).astype(bf16)
    for h in range(2):
        shared_send[h] = shared_part[:, 1024 * h : 1024 * (h + 1)]
    shared_copy = to_partner(shared_send.at[1 - tp], shared_recv, shared_sems.at[0], shared_sems.at[1])
    shared_copy.start()
    combine_rows(code, weight, comb)
    for h in range(4):
        forget_t[h] = forget[:, heads[h]].T
        key_t[h] = key[:, heads[h]].T
        input_h[h] = input_val[:, heads[h]]

    def update(h, c):
        keep, add, value = forget_t[h], key_t[h], input_h[h]
        for s in range(16):
            state_out[s, h] = keep[:, s : s + 1] * state_v[s, h] + add[:, s : s + 1] * value[s : s + 1, :]
        return c

    lax.fori_loop(0, 4, update, 0)
    out_row, in_row = iota((256, 256), 0), iota((256, 256), 1)
    sort = ((out_row // 32 == in_row % 8) & ((out_row // 2) % 16 == in_row // 16)
            & (out_row % 2 == (in_row // 8) % 2)).astype(bf16)
    unsort = ((in_row // 32 == out_row % 8) & ((in_row // 2) % 16 == out_row // 16)
              & (in_row % 2 == (out_row // 8) % 2)).astype(bf16)
    for copy in late[3:]:
        copy.wait()
    for g, blocks in ((1, range(1, 4)), (0, range(1))):
        group = pl.ds(16 * blocks[0], 16 * len(blocks) - g)
        mine = pl.ds(32 * blocks[0], 32 * len(blocks))
        to_partner(send.at[group], recv.at[group], go_send, go_recv.at[g]).wait_recv()
        for b in blocks:
            sorted_rows = dot(sort, recv[pl.ds(16 * b, 16)].reshape(256, 256)).astype(bf16)
            for j in range(8):
                xs[pl.ds(32 * b, 32), pl.ds(256 * j, 256)] = sorted_rows[32 * j : 32 * j + 32]
        x = xs[mine, :]
        hidden_own = (silu(dot(x, gate_own[...])) * dot(x, up_own[...])).astype(bf16)
        if g == 1:
            for copy in pushes:
                copy.wait()
        hidden_par = (silu(dot(x, gate_par[...])) * dot(x, up_par[...])).astype(bf16)
        for n in range(8):
            cols = pl.ds(256 * n, 256)
            xs[mine, cols] = (dot(hidden_own, down_own[:, cols]) + dot(hidden_par, down_par[:, cols])).astype(bf16)
        for b in blocks:
            tall = jnp.concatenate(
                [
                    jnp.concatenate(
                        [xs[pl.ds(32 * b, 32), pl.ds(128 * j + 1024 * h, 128)] for h in range(2)], axis=1
                    )
                    for j in range(8)
                ],
                axis=0,
            )
            turned = dot(unsort, tall).astype(bf16)
            for i in range(16):
                p = 16 * b + i
                for h in range(2):
                    ret[2 * p + h] = turned[16 * i : 16 * i + 16, 128 * h : 128 * h + 128]
                    if p < 63:
                        pltpu.make_async_remote_copy(
                            src_ref=ret.at[2 * p + h], dst_ref=back.at[2 * p + tp], send_sem=ret_send,
                            recv_sem=ret_recv, device_id=(peers.behind(p), h), device_id_type=MESH,
                        ).start()
    to_partner(ret.at[127 - tp], back.at[126 + tp], ret_send, ret_recv).start()
    back[126 + tp] = ret[126 + tp]
    shared_copy.wait()
    base_out[...] = residual_v[tp] + (shared_send[tp].astype(f32) + shared_recv[...].astype(f32)).astype(bf16).astype(f32)
    to_partner(all_of(send, 63), all_of(recv, 63), go_send, go_recv.at[0]).wait_send()
    to_partner(all_of(ret, 127), all_of(back, 127), ret_send, ret_recv).wait()


def finish_kernel(state_ref, back_ref, comb_ref, base_ref, out_hbm, state_hbm, out_v, sems):
    state_copy = pltpu.make_async_copy(state_ref, state_hbm, sems.at[0])
    state_copy.start()
    total = dot(comb_ref[...], back_ref[...].reshape(2048, 128))
    for j in range(8):
        cols = slice(128 * j, 128 * (j + 1))
        out_v[:, cols] = (base_ref[:, cols] + total[16 * j : 16 * j + 16]).astype(bf16)
    out_copy = pltpu.make_async_copy(out_v, out_hbm, sems.at[1])
    out_copy.start()
    out_copy.wait()
    state_copy.wait()


def local(
    tokens, state, mix_gain, moe_gain, head_gain, w_forget, w_query, w_input, w_outgate, lower_bound, w_mix_out,
    routes, route_scores, expert_gate, expert_up, expert_down, shared_gate, shared_up, shared_down,
):
    vm = pl.BlockSpec(memory_space=pltpu.VMEM)
    hbm = pl.BlockSpec(memory_space=pltpu.HBM)
    dma = pltpu.SemaphoreType.DMA

    def buf(*shape, dtype=bf16):
        return pltpu.VMEM(shape, dtype)

    kept = pl.pallas_call(
        layer_kernel,
        name="layer",
        out_shape=(
            buf(16, 4, 128, 128, dtype=f32), buf(128, 16, 128), buf(128, 2048), buf(16, 1024, dtype=f32)
        ),
        in_specs=[hbm] * 20,
        out_specs=(vm,) * 4,
        scratch_shapes=[
            buf(16, 2048), buf(1, 2048, dtype=f32), buf(1, 2048, dtype=f32), buf(1, 128, dtype=f32),
            buf(1, 512, dtype=f32), buf(6, 16, dtype=i32), buf(6, 16, dtype=f32), buf(64, 16, dtype=i32),
            buf(2048, 512), buf(2048, 512), buf(2048, 512), buf(2048, 512), buf(16, 4, 128, 128, dtype=f32),
            buf(512, 2048), buf(2048, 256), buf(2048, 256), buf(256, 2048),
            buf(2048, 256), buf(2048, 256), buf(256, 2048), buf(2048, 256), buf(2048, 256), buf(256, 2048),
            buf(16, 2048), buf(16, 2048), buf(2, 16, 1024), buf(16, 1024), buf(2, 16, 1024, dtype=f32),
            buf(4, 128, 16, dtype=f32), buf(4, 128, 16, dtype=f32), buf(4, 16, 128, dtype=f32),
            buf(1024, 128), buf(64, 16, 256), buf(64, 16, 256), buf(128, 2048), buf(128, 16, 128),
            dma((8,)), dma((8,)), dma((4,)), dma((2,)), dma((6,)), dma((3,)), dma((3,)), dma((2,)), dma((2,)), dma, dma((2,)), dma, dma,
        ],
        compiler_params=pltpu.CompilerParams(
            collective_id=0, has_side_effects=True, vmem_limit_bytes=vmem_all - (5 << 20) - (160 << 10)
        ),
    )(
        tokens, state, mix_gain.reshape(1, -1), moe_gain.reshape(1, -1), head_gain.reshape(1, -1),
        w_forget, w_query, w_input, w_outgate, lower_bound.reshape(1, -1), w_mix_out,
        routes.T, route_scores.T, expert_gate, expert_up, expert_down, shared_gate, shared_up, shared_down,
        jnp.asarray(np.repeat(np.array(order, np.int32)[:, None], 16, 1)),
    )
    return pl.pallas_call(
        finish_kernel,
        name="finish",
        out_shape=(jax.ShapeDtypeStruct((16, 1024), bf16), jax.ShapeDtypeStruct((16, 4, 128, 128), f32)),
        in_specs=[vm] * 4,
        out_specs=(hbm, hbm),
        scratch_shapes=[buf(16, 1024), dma((2,))],
        compiler_params=pltpu.CompilerParams(vmem_limit_bytes=8 << 20),
    )(*kept)


def solution(mesh):
    return jax.shard_map(
        local,
        mesh=mesh,
        in_specs=(
            P("ep", None),
            P("ep", "tp", None, None),
            P(),
            P(),
            P(),
            P(None, "tp"),
            P(None, "tp"),
            P(None, "tp"),
            P(None, "tp"),
            P("tp"),
            P("tp", None),
            P("ep", None),
            P("ep", None),
            P("ep", None, "tp"),
            P("ep", None, "tp"),
            P("ep", "tp", None),
            P(None, "tp"),
            P(None, "tp"),
            P("tp", None),
        ),
        out_specs=(P("ep", "tp"), P("ep", "tp", None, None)),
        check_vma=False,
    )
```
